128 devices in a mesh: ep: 32 (over z, y, core), tp: 4 (over x).
Axes of the slice: x: 4, y: 4, z: 4, core: 2. Of those that a mesh axis runs over, the one named last changes fastest.
Arguments:
- tokens: bfloat16 [16384, 2048], P(('ep', 'tp')), may hold values from -6 to 6
- norm_gain: float32 [2048], replicated, may hold values from 0.1 to 1.9
- w_gate: bfloat16 [128, 2048, 512], P(('ep', 'tp')), may hold values from -0.125 to 0.125
- w_up: bfloat16 [128, 2048, 512], P(('ep', 'tp')), may hold values from -0.125 to 0.125
- w_down: bfloat16 [128, 512, 2048], P(('ep', 'tp')), may hold values from -0.25 to 0.25
- routing: int32 [16384, 2], P(('ep', 'tp')), may hold values from 0 to 127, as said below
- gate_weight: float32 [16384, 2], P(('ep', 'tp')), may hold values from 0.05 to 1
Outputs:
- combined: bfloat16 [16384, 2048], P(('ep', 'tp'))
The draws below stay inside these ranges and needn't reach their ends.
Inputs may be any that keep to these rules, and one draw needn't show every extreme that they name: `routing`: A token's 2 experts are distinct and lie in one group of 4 consecutive experts. Of the 128 tokens of each device exactly 4 choose each group; no expert is named by more than 4 tokens of one device, and in every group one expert is named by exactly 4 tokens of every device.
All inputs are finite; a program needn't handle non-finite values.
Results may differ from the reference program's by a relative error of at most 0.0085.
Values may be sent and summed in bfloat16 or wider, within the bound.
A program may use at most 64 MiB of HBM per device.

```python
import math
import jax
import jax.numpy as jnp
from jax import lax

D = 2048
FF = 512
GROUP_EXPERTS = 4
TOP = 2
TOK_DEV = 128
EXPERTS = 128
GROUPS = 32
CAP = 4
TOKENS = 16384


def draw_routing(key, part):
    source_count = TOKENS // TOK_DEV
    heavy_key = jax.random.fold_in(key, 11)
    cut_key = jax.random.fold_in(key, 12)
    shuffle_key = jax.random.fold_in(key, 13)
    heavy_member = jax.random.randint(heavy_key, (GROUPS,), 0, GROUP_EXPERTS)
    cut_points = jax.random.randint(cut_key, (source_count, GROUPS, 2), 0, CAP + 1)
    lower = jnp.min(cut_points, axis=-1)
    higher = jnp.max(cut_points, axis=-1)
    rest_loads = jnp.stack([lower, higher - lower, CAP - higher], axis=-1)
    members = jnp.arange(GROUP_EXPERTS, dtype=jnp.int32)
    is_heavy = members[None, :] == heavy_member[:, None]
    rank = jnp.clip(members[None, :] - (members[None, :] > heavy_member[:, None]).astype(jnp.int32), 0, 2)
    rank_full = jnp.broadcast_to(rank[None], (source_count, GROUPS, GROUP_EXPERTS))
    load_table = jnp.where(is_heavy[None], CAP, jnp.take_along_axis(rest_loads, rank_full, axis=2))
    bounds = jnp.cumsum(load_table, axis=-1)
    entries = jnp.arange(2 * CAP, dtype=jnp.int32)
    local_ident = jnp.sum((entries[None, None, :, None] >= bounds[:, :, None, :GROUP_EXPERTS - 1]).astype(jnp.int32), axis=-1)
    group_base = jnp.arange(GROUPS, dtype=jnp.int32) * GROUP_EXPERTS
    pair_table = jnp.stack([local_ident[:, :, :CAP], local_ident[:, :, CAP:]], axis=-1) + group_base[None, :, None, None]
    pair_table = pair_table.reshape(source_count, TOK_DEV, TOP)
    shuffles = jax.vmap(lambda subkey: jax.random.permutation(subkey, TOK_DEV))(jax.random.split(shuffle_key, source_count))
    routing = jnp.take_along_axis(pair_table, shuffles[:, :, None].astype(jnp.int32), axis=1)
    return routing.reshape(TOKENS, TOP).astype(jnp.int32)


def level_of(rng, shape, shards, low, top_value):
    level, own = 1.0, jax.random.fold_in(rng, 6)
    for dim, blocks in shards:
        steps = jnp.exp(jax.random.uniform(jax.random.fold_in(own, dim), (blocks,), jnp.float32, low / len(shards), top_value / len(shards)))
        level = level * jnp.repeat(steps, shape[dim] // blocks).reshape([-1 if axis == dim else 1 for axis in range(len(shape))])
    return level


def gaussian(rng, shape, spread, most, cuts=(), kind=jnp.bfloat16):
    values = spread * jax.random.normal(rng, shape, jnp.float32)
    if cuts:
        values = values * level_of(rng, shape, cuts, -0.22, 0.18)
    return jnp.clip(values, -most, most).astype(kind)


def setup_inputs(seed: int = 0) -> dict:
    key_list = jax.random.split(jax.random.key(seed), 8)
    tokens = gaussian(key_list[0], (TOKENS, D), 1.0, 6.0, ((0, 128),))
    norm_gain = jnp.clip(1.0 + 0.18 * jax.random.normal(key_list[1], (D,), jnp.float32), 0.1, 1.9)
    w_gate = gaussian(key_list[2], (EXPERTS, D, FF), D ** -0.5, 0.125, ((0, 128),))
    w_up = gaussian(key_list[3], (EXPERTS, D, FF), D ** -0.5, 0.125, ((0, 128),))
    w_down = gaussian(key_list[4], (EXPERTS, FF, D), FF ** -0.5, 0.25, ((0, 128),))
    routing = draw_routing(jax.random.fold_in(key_list[7], 71), 0)
    gate_weight = jnp.clip(jnp.exp(math.log(1.0) - 2.9957323 * jax.random.uniform(key_list[6], (TOKENS, TOP), jnp.float32) ** level_of(key_list[6], (TOKENS, TOP), ((0, 128),), -0.2, 0.2)), 0.05, 1.0)
    return {"tokens": tokens, "norm_gain": norm_gain, "w_gate": w_gate, "w_up": w_up, "w_down": w_down, "routing": routing, "gate_weight": gate_weight}


def reference(tokens, norm_gain, w_gate, w_up, w_down, routing, gate_weight):
    source_count = TOKENS // TOK_DEV
    values = tokens.astype(jnp.float32)
    scale = lax.rsqrt(lax.optimization_barrier(jnp.mean(values * values, axis=-1, keepdims=True)) + 1e-06)
    normed = (values * scale * norm_gain.astype(jnp.float32)).astype(jnp.bfloat16)
    assigned = routing.reshape(source_count, TOK_DEV * TOP).astype(jnp.int32)

    def count_slots(block):
        onehot = (block[:, None] == jnp.arange(EXPERTS, dtype=jnp.int32)[None, :]).astype(jnp.int32)
        running = jnp.cumsum(onehot, axis=0)
        return lax.optimization_barrier(jnp.sum(onehot * running, axis=1)) - 1
    slot_index = lax.map(count_slots, assigned)
    source_index = jnp.arange(source_count, dtype=jnp.int32)[:, None]
    position = (assigned * source_count + source_index) * CAP + slot_index
    dump_index = TOKENS * TOP
    slot_owner = jnp.full((EXPERTS * source_count * CAP,), dump_index, jnp.int32)
    slot_owner = slot_owner.at[position.reshape(-1)].set(jnp.arange(TOKENS * TOP, dtype=jnp.int32))
    slot_owner = slot_owner.reshape(EXPERTS, source_count * CAP)
    normed_pad = jnp.concatenate([normed, jnp.zeros((1, D), jnp.bfloat16)], axis=0)

    def one_expert(expert, results):
        owners = lax.dynamic_index_in_dim(slot_owner, expert, 0, keepdims=False)
        slot_rows = normed_pad[owners // TOP]
        gate_part = jnp.dot(slot_rows, lax.dynamic_index_in_dim(w_gate, expert, 0, keepdims=False), preferred_element_type=jnp.float32)
        up_part = jnp.dot(slot_rows, lax.dynamic_index_in_dim(w_up, expert, 0, keepdims=False), preferred_element_type=jnp.float32)
        hidden = (jax.nn.silu(gate_part) * up_part).astype(jnp.bfloat16)
        expert_out = jnp.dot(hidden, lax.dynamic_index_in_dim(w_down, expert, 0, keepdims=False), preferred_element_type=jnp.float32).astype(jnp.bfloat16)
        return results.at[owners].set(expert_out)
    results = lax.fori_loop(0, EXPERTS, one_expert, jnp.zeros((TOKENS * TOP + 1, D), jnp.bfloat16))
    picked = results[:TOKENS * TOP].reshape(TOKENS, TOP, D).astype(jnp.float32)
    return lax.optimization_barrier(jnp.sum(gate_weight.astype(jnp.float32)[:, :, None] * picked, axis=1)).astype(jnp.bfloat16)
```

```python
import functools

import jax
import jax.numpy as jnp
from jax import lax
from jax.experimental import pallas as pl
from jax.experimental.pallas import tpu as pltpu
from jax.sharding import PartitionSpec as P

MESH = pl.DeviceIdType.MESH
F32, BF16, I32 = jnp.float32, jnp.bfloat16, jnp.int32
HIGHEST = lax.Precision.HIGHEST

PAIRS = (
    (0, 0), (0, 1), (0, 3), (1, 0),
    (0, 2), (2, 0), (3, 1), (1, 2),
    (2, 2), (2, 1), (2, 3), (3, 2),
    (3, 0), (1, 1), (3, 3), (1, 3),
)
SLOTS = 32
CHUNKS = 4
PER = SLOTS // CHUNKS
HALF = PER // 2
CAP = 4
QUART = 4
BLOCK = CAP * QUART
AGA, AGB, FWD, RS1, RS2A, RS2B = range(6)
RIGHT, LEFT = 0, 1


def iota(shape, dim):
    return lax.broadcasted_iota(I32, shape, dim)


def onehot(mask):
    return jnp.where(mask, 1.0, 0.0).astype(BF16)


def kernel(tok_ref, gain_ref, wg_hbm, wu_hbm, wd_hbm, route_ref, gw_ref, out_ref,
           wg, wu, wd, stack, place, unplace, spread, gather, msgs, meta_out, xbuf, xmeta, mrows, gall,
           rows, ybuf, cbuf, rs1, rs2, back, ret,
           w_sem, y_send, y_recv, m_send, m_recv, x_send, x_recv, xm_send, xm_recv, b_send, b_recv):
    tokens, width = tok_ref.shape
    part = width // QUART
    me = lax.axis_index("ep")
    mx = lax.axis_index("tp")
    z, y, c = me // 8, (me // 2) % 4, me % 2
    right = {"tp": (mx + 1) % 4}
    left = {"tp": (mx + 3) % 4}

    def peer(slot, sign):
        dz, dy = PAIRS[slot // 2]
        dc = slot % 2
        return {"ep": ((z + 4 + sign * dz) % 4) * 8 + ((y + 4 + sign * dy) % 4) * 2 + (c + dc) % 2}

    weights = [pltpu.make_async_copy(src.at[0], dst, w_sem.at[n])
               for n, (src, dst) in enumerate(((wg_hbm, wg), (wu_hbm, wu), (wd_hbm, wd)))]
    for copy in weights:
        copy.start()

    barrier = pltpu.get_barrier_semaphore()
    for slot in range(1, SLOTS):
        pl.semaphore_signal(barrier, inc=1, device_id=peer(slot, -1), device_id_type=MESH)
    for side in (right, left):
        pl.semaphore_signal(barrier, inc=1, device_id=side, device_id_type=MESH)

    values = tok_ref[...].astype(F32)
    scale = lax.rsqrt(jnp.mean(values * values, axis=-1, keepdims=True) + 1e-06)
    normed = (values * scale * gain_ref[...]).astype(BF16)
    for q in range(QUART):
        stack[q * tokens:(q + 1) * tokens, :] = normed[:, q * part:(q + 1) * part]

    first = route_ref[:, 0:1]
    second = route_ref[:, 1:2]
    square = jnp.broadcast_to((first // 4).astype(F32), (tokens, tokens))
    turned = square.T
    same = square == turned
    row_id, col_id = iota((tokens, tokens), 0), iota((tokens, tokens), 1)
    rank_col = jnp.sum(jnp.where(same & (col_id < row_id), 1, 0), axis=1, keepdims=True)
    rank_row = jnp.sum(jnp.where(same & (row_id < col_id), 1, 0), axis=0, keepdims=True)

    def slot_of(group):
        rel = ((z + 4 - group // 8) % 4) * 4 + (y + 4 - (group // 2) % 4) % 4
        pair = jnp.zeros_like(group)
        for n, (dz, dy) in enumerate(PAIRS):
            pair = pair + jnp.where(rel == dz * 4 + dy, n, 0)
        return pair * 2 + (group + c) % 2

    slot_col = slot_of(first // 4)
    slot_row = slot_of(turned[0:1, :].astype(I32))
    pos_col = slot_col * CAP + rank_col
    pos_row = slot_row * CAP + rank_row

    r = iota((SLOTS * BLOCK, tokens), 0)
    place_of_r = (r // BLOCK) * CAP + r % CAP
    hit = place_of_r == pos_row
    for q in range(QUART):
        place[:, q * tokens:(q + 1) * tokens] = onehot(hit & ((r // CAP) % QUART == q))
    msgs[...] = jnp.dot(place[...], stack[...], preferred_element_type=F32).astype(BF16).reshape(SLOTS, BLOCK, part)
    xbuf[0, 0] = msgs[0]

    lane = iota((tokens, 128), 1)
    of_lane = (jnp.where(first % 4 == lane % 4, gw_ref[:, 0:1], 0.0)
               + jnp.where(second % 4 == lane % 4, gw_ref[:, 1:2], 0.0))
    of_lane = jnp.where(rank_col == lane // 4, of_lane, 0.0)
    chosen = jnp.where(iota((SLOTS, tokens), 0) == slot_row, 1.0, 0.0)
    meta = jnp.dot(chosen, of_lane, preferred_element_type=F32, precision=HIGHEST)
    for slot in range(SLOTS):
        meta_out[slot] = meta[slot:slot + 1, :]
    xmeta[0, 0] = meta[0:1, :]

    pl.semaphore_wait(barrier, SLOTS + 1)

    def remote(src, dst, send, recv, device):
        return pltpu.make_async_remote_copy(src_ref=src, dst_ref=dst, send_sem=send, recv_sem=recv,
                                            device_id=device, device_id_type=MESH)

    for slot in range(1, SLOTS):
        remote(msgs.at[slot], xbuf.at[0, slot], y_send.at[slot // PER], y_recv.at[slot // PER], peer(slot, -1)).start()
        if slot == PER - 1:
            for other in range(1, SLOTS):
                remote(meta_out.at[other], xmeta.at[0, other], m_send, m_recv, peer(other, -1)).start()

    half = 2 * PER * BLOCK
    a, b = iota((half, half), 0), iota((half, half), 1)
    piece = PER * BLOCK
    run = PER * CAP

    def other_order(n):
        return (n // piece) * piece + ((n % run) // CAP) * BLOCK + ((n % piece) // run) * CAP + n % CAP
    spread[...] = onehot(other_order(a) == b)
    gather[...] = onehot(other_order(b) == a)
    r = iota((tokens, SLOTS * BLOCK), 1)
    hit = (r // BLOCK) * CAP + r % CAP == pos_col
    for q in range(QUART):
        unplace[q * tokens:(q + 1) * tokens, :] = onehot(hit & ((r // CAP) % QUART == q))

    def lo(j):
        return slice(j * PER, j * PER + HALF)

    def hi(j):
        return slice(j * PER + HALF, (j + 1) * PER)

    def both(j):
        return slice(j * PER, (j + 1) * PER)

    def ag(side, kind, j):
        part_of = lo(j) if kind == AGA else hi(j)
        to = 1 if side == RIGHT else 3
        return remote(xbuf.at[0, part_of], xbuf.at[to, part_of], x_send.at[side, kind, j], x_recv.at[side, kind, j],
                      right if side == RIGHT else left)

    def fwd(side, j):
        part_of, held = (lo(j), 1) if side == RIGHT else (hi(j), 3)
        return remote(xbuf.at[held, part_of], xbuf.at[2, part_of], x_send.at[side, FWD, j], x_recv.at[side, FWD, j],
                      right if side == RIGHT else left)

    def rs_first(side, j):
        part_of = lo(j) if side == RIGHT else hi(j)
        return remote(cbuf.at[2, part_of], rs1.at[side, j], x_send.at[side, RS1, j], x_recv.at[side, RS1, j],
                      right if side == RIGHT else left)

    def rs_second(side, kind, j):
        part_of = lo(j) if kind == RS2A else hi(j)
        held = 3 if side == RIGHT else 1
        return remote(cbuf.at[held, part_of], rs2.at[side, part_of], x_send.at[side, kind, j], x_recv.at[side, kind, j],
                      right if side == RIGHT else left)

    def start_gather(j):
        src = xbuf.at[0, slice(j * PER + (1 if j == 0 else 0), (j + 1) * PER)]
        remote(src, src, y_send.at[j], y_recv.at[j], right).wait_recv()
        ag(RIGHT, AGA, j).start()
        ag(LEFT, AGB, j).start()
        ag(RIGHT, AGB, j).start()
        ag(LEFT, AGA, j).start()

    def forward(j):
        ag(RIGHT, AGA, j).wait_recv()
        fwd(RIGHT, j).start()
        ag(LEFT, AGB, j).wait_recv()
        fwd(LEFT, j).start()

    def meta_gather():
        src = xmeta.at[0, slice(1, SLOTS)]
        remote(src, src, m_send, m_recv, right).wait_recv()
        remote(xmeta.at[0], xmeta.at[1], xm_send.at[0], xm_recv.at[0], right).start()
        remote(xmeta.at[0], xmeta.at[3], xm_send.at[1], xm_recv.at[1], left).start()

    def meta_forward():
        remote(xmeta.at[0], xmeta.at[1], xm_send.at[0], xm_recv.at[0], right).wait_recv()
        remote(xmeta.at[1], xmeta.at[2], xm_send.at[2], xm_recv.at[2], right).start()
        remote(xmeta.at[0], xmeta.at[3], xm_send.at[1], xm_recv.at[1], left).wait_recv()

    def meta_use():
        remote(xmeta.at[1], xmeta.at[2], xm_send.at[2], xm_recv.at[2], right).wait_recv()
        for side in range(4):
            for slot in range(SLOTS):
                mrows[side * SLOTS + slot:side * SLOTS + slot + 1, :] = xmeta[side, slot]
        n = iota((CHUNKS * 4 * run, 4 * SLOTS), 0)
        col = iota((CHUNKS * 4 * run, 4 * SLOTS), 1)
        source = ((n // run) % 4) * SLOTS + (n // (4 * run)) * PER + (n % run) // CAP
        picked = jnp.dot(jnp.where(source == col, 1.0, 0.0), mrows[...], preferred_element_type=F32, precision=HIGHEST)
        mine = (n % CAP) * 4 + mx == col
        gall[...] = jnp.broadcast_to(jnp.sum(jnp.where(mine, picked, 0.0), axis=1, keepdims=True), gall.shape)

    def compute(j):
        ag(RIGHT, AGB, j).wait_recv()
        ag(LEFT, AGA, j).wait_recv()
        fwd(RIGHT, j).wait_recv()
        fwd(LEFT, j).wait_recv()
        for pair in range(2):
            block = xbuf[2 * pair:2 * pair + 2, both(j)].reshape(half, part)
            ordered = jnp.dot(spread[...], block, preferred_element_type=F32).astype(BF16)
            for side in range(2):
                for q in range(QUART):
                    at = (2 * pair + side) * run
                    rows[at:at + run, q * part:(q + 1) * part] = ordered[side * piece + q * run:side * piece + (q + 1) * run]
        if j == 0:
            weights[0].wait()
            weights[1].wait()
        gate = jnp.dot(rows[...], wg[...], preferred_element_type=F32)
        up = jnp.dot(rows[...], wu[...], preferred_element_type=F32)
        hidden = (gate / (1.0 + jnp.exp(-gate)) * up).astype(BF16)
        if j == 0:
            weights[2].wait()
            meta_use()
        weight = gall[j * 4 * run:(j + 1) * 4 * run, 0:1]
        for q in range(QUART):
            piece_out = jnp.dot(hidden, wd[:, q * part:(q + 1) * part], preferred_element_type=F32)
            piece_out = (piece_out * weight).astype(BF16)
            for side in range(4):
                ybuf[side * piece + q * run:side * piece + (q + 1) * run, :] = piece_out[side * run:(side + 1) * run]
        for pair in (1, 0):
            block = jnp.dot(gather[...], ybuf[pair * half:(pair + 1) * half, :], preferred_element_type=F32).astype(BF16)
            cbuf[2 * pair:2 * pair + 2, both(j)] = block.reshape(2, PER, BLOCK, part)
            if pair == 1:
                rs_first(RIGHT, j).start()
                rs_first(LEFT, j).start()
        rs_second(RIGHT, RS2B, j).start()
        rs_second(LEFT, RS2A, j).start()

    def reduce_first(j):
        rs_first(RIGHT, j).wait_recv()
        cbuf[3, lo(j)] = (cbuf[3, lo(j)].astype(F32) + rs1[RIGHT, j].astype(F32)).astype(BF16)
        rs_second(RIGHT, RS2A, j).start()
        rs_first(LEFT, j).wait_recv()
        cbuf[1, hi(j)] = (cbuf[1, hi(j)].astype(F32) + rs1[LEFT, j].astype(F32)).astype(BF16)
        rs_second(LEFT, RS2B, j).start()

    def give_back(j):
        for side in (RIGHT, LEFT):
            rs_second(side, RS2A, j).wait_recv()
            rs_second(side, RS2B, j).wait_recv()
        total = cbuf[0, both(j)].astype(F32) + rs2[RIGHT, both(j)].astype(F32) + rs2[LEFT, both(j)].astype(F32)
        back[both(j)] = total.astype(BF16)
        if j == 0:
            ret[0] = back[0]
        for slot in range(max(1, j * PER), (j + 1) * PER):
            remote(back.at[slot], ret.at[slot], b_send.at[j], b_recv.at[j], peer(slot, 1)).start()

    start_gather(0)
    start_gather(1)
    forward(0)
    meta_gather()
    start_gather(2)
    forward(1)
    meta_forward()
    compute(0)
    start_gather(3)
    forward(2)
    compute(1)
    reduce_first(0)
    forward(3)
    compute(2)
    reduce_first(1)
    give_back(0)
    compute(3)
    reduce_first(2)
    give_back(1)
    reduce_first(3)
    give_back(2)
    give_back(3)

    for j in range(CHUNKS):
        src = ret.at[slice(j * PER + (1 if j == 0 else 0), (j + 1) * PER)]
        remote(src, src, b_send.at[j], b_recv.at[j], right).wait_recv()
    result = jnp.dot(unplace[...], ret[...].reshape(SLOTS * BLOCK, part), preferred_element_type=F32).astype(BF16)
    for q in range(QUART):
        out_ref[:, q * part:(q + 1) * part] = result[q * tokens:(q + 1) * tokens]

    for j in range(CHUNKS):
        src = msgs.at[slice(j * PER + (1 if j == 0 else 0), (j + 1) * PER)]
        remote(src, src, y_send.at[j], y_recv.at[j], right).wait_send()
        remote(src, src, b_send.at[j], b_recv.at[j], right).wait_send()
        for side in (RIGHT, LEFT):
            ag(side, AGA, j).wait_send()
            ag(side, AGB, j).wait_send()
            fwd(side, j).wait_send()
            rs_first(side, j).wait_send()
            rs_second(side, RS2A, j).wait_send()
            rs_second(side, RS2B, j).wait_send()
    src = meta_out.at[slice(1, SLOTS)]
    remote(src, src, m_send, m_recv, right).wait_send()
    for n in range(3):
        remote(xmeta.at[0], xmeta.at[1], xm_send.at[n], xm_recv.at[n], right).wait_send()


def local(tokens, norm_gain, w_gate, w_up, w_down, routing, gate_weight):
    count, width = tokens.shape
    hidden = w_gate.shape[2]
    part = width // QUART
    total = SLOTS * BLOCK
    vmem = pl.BlockSpec(memory_space=pltpu.VMEM)
    hbm = pl.BlockSpec(memory_space=pltpu.HBM)
    dma = pltpu.SemaphoreType.DMA
    return pl.pallas_call(
        kernel,
        out_shape=jax.ShapeDtypeStruct((count, width), BF16),
        in_specs=[vmem, vmem, hbm, hbm, hbm, vmem, vmem],
        out_specs=vmem,
        scratch_shapes=[
            pltpu.VMEM((width, hidden), BF16),
            pltpu.VMEM((width, hidden), BF16),
            pltpu.VMEM((hidden, width), BF16),
            pltpu.VMEM((QUART * count, part), BF16),
            pltpu.VMEM((total, QUART * count), BF16),
            pltpu.VMEM((QUART * count, total), BF16),
            pltpu.VMEM((2 * PER * BLOCK, 2 * PER * BLOCK), BF16),
            pltpu.VMEM((2 * PER * BLOCK, 2 * PER * BLOCK), BF16),
            pltpu.VMEM((SLOTS, BLOCK, part), BF16),
            pltpu.VMEM((SLOTS, 1, 128), F32),
            pltpu.VMEM((4, SLOTS, BLOCK, part), BF16),
            pltpu.VMEM((4, SLOTS, 1, 128), F32),
            pltpu.VMEM((4 * SLOTS, 128), F32),
            pltpu.VMEM((4 * SLOTS * CAP, 128), F32),
            pltpu.VMEM((4 * PER * CAP, width), BF16),
            pltpu.VMEM((4 * PER * BLOCK, part), BF16),
            pltpu.VMEM((4, SLOTS, BLOCK, part), BF16),
            pltpu.VMEM((2, CHUNKS, HALF, BLOCK, part), BF16),
            pltpu.VMEM((2, SLOTS, BLOCK, part), BF16),
            pltpu.VMEM((SLOTS, BLOCK, part), BF16),
            pltpu.VMEM((SLOTS, BLOCK, part), BF16),
            dma((3,)), dma((CHUNKS,)), dma((CHUNKS,)), dma, dma,
            dma((2, 6, CHUNKS)), dma((2, 6, CHUNKS)), dma((3,)), dma((3,)), dma((CHUNKS,)), dma((CHUNKS,)),
        ],
        compiler_params=pltpu.CompilerParams(
            collective_id=0, has_side_effects=True, vmem_limit_bytes=56 * 1024 * 1024
        ),
    )(tokens, norm_gain.reshape(1, width), w_gate, w_up, w_down, routing, gate_weight)


def solution(mesh):
    placed = (
        P(("ep", "tp"), None),
        P(),
        P(("ep", "tp"), None, None),
        P(("ep", "tp"), None, None),
        P(("ep", "tp"), None, None),
        P(("ep", "tp"), None),
        P(("ep", "tp"), None),
    )
    return jax.shard_map(
        local, mesh=mesh, in_specs=placed, out_specs=P(("ep", "tp"), None), check_vma=False
    )
```

```python
import functools

import jax
import jax.numpy as jnp
from jax import lax
from jax.experimental import pallas as pl
from jax.experimental.pallas import tpu as pltpu
from jax.sharding import PartitionSpec as P

MESH = pl.DeviceIdType.MESH
F32, BF16, I32 = jnp.float32, jnp.bfloat16, jnp.int32
HIGHEST = lax.Precision.HIGHEST

CHUNKS = {
    "E": ((0, 0),),
    "A": ((0, 1), (0, 3), (1, 0), (3, 0)),
    "B": ((2, 0), (2, 1), (0, 2), (1, 2)),
    "D": ((1, 1), (3, 3), (1, 3)),
    "C": ((2, 2), (2, 3), (3, 2), (3, 1)),
}
NAMES = tuple(CHUNKS)
DIRECT = "EA"
PAIRS = tuple(pair for name in NAMES for pair in CHUNKS[name])
SLOTS = 2 * len(PAIRS)
COUNT = {name: 2 * len(CHUNKS[name]) for name in NAMES}
START = {name: 2 * PAIRS.index(CHUNKS[name][0]) for name in NAMES}
CAP = 4
QUART = 4
BLOCK = CAP * QUART
AGA, AGB, FWD, RS1, RS2A, RS2B = range(6)
RIGHT, LEFT = 0, 1
SIZES = tuple(sorted(set(COUNT.values())))
ORDER = (
    "dE", "oD", "dA", "oB", "oC", "k", "fE", "gD", "fA", "mS", "gB", "fD", "gC", "fB", "mU", "fC",
    "cD", "cB", "cC", "rB", "rC", "cA", "rD", "cE", "bB", "bC", "rA", "bD", "rE", "bA", "bE",
)


def iota(shape, dim):
    return lax.broadcasted_iota(I32, shape, dim)


def onehot(mask):
    return jnp.where(mask, 1.0, 0.0).astype(BF16)


def kernel(tok_hbm, gain_hbm, wg_hbm, wu_hbm, wd_hbm, route_hbm, gw_hbm, out_ref,
           tok_ref, gain_ref, route_ref, gw_ref, wg, wu, wd, stack, place, unplace, spreads, gathers, msgs, meta_out, xbuf, xmeta, mrows, gall,
           rows, ybuf, cbuf, rs1, rs2, back, ret,
           w_sem, y_send, y_recv, m_send, m_recv, x_send, x_recv, xm_send, xm_recv, b_send, b_recv):
    tokens, width = tok_ref.shape
    part = width // QUART
    me = lax.axis_index("ep")
    mx = lax.axis_index("tp")
    z, y, c = me // 8, (me // 2) % 4, me % 2
    right = {"tp": (mx + 1) % 4}
    left = {"tp": (mx + 3) % 4}

    def peer(slot, sign, dx=0):
        dz, dy = PAIRS[slot // 2]
        dc = slot % 2
        group = ((z + 4 + sign * dz) % 4) * 8 + ((y + 4 + sign * dy) % 4) * 2 + (c + dc) % 2
        return {"ep": group, "tp": (mx + 4 + dx) % 4}

    def slots_of(name):
        return range(START[name], START[name] + COUNT[name])

    small = [pltpu.make_async_copy(src, dst, w_sem.at[3 + n]) for n, (src, dst) in enumerate((
        (tok_hbm, tok_ref), (gain_hbm, gain_ref), (route_hbm, route_ref), (gw_hbm, gw_ref)))]
    for copy in small:
        copy.start()
    weights = [pltpu.make_async_copy(src.at[0], dst, w_sem.at[n])
               for n, (src, dst) in enumerate(((wg_hbm, wg), (wu_hbm, wu), (wd_hbm, wd)))]

    barrier = pltpu.get_barrier_semaphore()
    for slot in range(1, SLOTS):
        pl.semaphore_signal(barrier, inc=1, device_id=peer(slot, -1), device_id_type=MESH)
    near = [slot for name in DIRECT for slot in slots_of(name) if slot]
    for slot in near:
        for dx in (1, -1):
            pl.semaphore_signal(barrier, inc=1, device_id=peer(slot, -1, dx), device_id_type=MESH)
    for side in (right, {"tp": (mx + 2) % 4}, left):
        pl.semaphore_signal(barrier, inc=1, device_id=side, device_id_type=MESH)

    for copy in small:
        copy.wait()
    for copy in weights:
        copy.start()
    values = tok_ref[...].astype(F32)
    scale = lax.rsqrt(jnp.mean(values * values, axis=-1, keepdims=True) + 1e-06)
    normed = (values * scale * gain_ref[...]).astype(BF16)
    for q in range(QUART):
        stack[q * tokens:(q + 1) * tokens, :] = normed[:, q * part:(q + 1) * part]

    first = route_ref[0:1, :]
    second = route_ref[1:2, :]
    group = first // 4
    square = jnp.broadcast_to(group.astype(F32), (tokens, tokens))
    earlier = (square.T == square) & (iota((tokens, tokens), 0) < iota((tokens, tokens), 1))
    rank = jnp.sum(jnp.where(earlier, 1, 0), axis=0, keepdims=True)

    def slot_of(group):
        rel = ((z + 4 - group // 8) % 4) * 4 + (y + 4 - (group // 2) % 4) % 4
        pair = jnp.zeros_like(group)
        for n, (dz, dy) in enumerate(PAIRS):
            pair = pair + jnp.where(rel == dz * 4 + dy, n, 0)
        return pair * 2 + (group + c) % 2

    slot_row = slot_of(group)
    pos_row = slot_row * CAP + rank
    pos_col = jnp.broadcast_to(pos_row.astype(F32), (tokens, tokens)).T[:, 0:1].astype(I32)

    r = iota((SLOTS * BLOCK, tokens), 0)
    place_of_r = (r // BLOCK) * CAP + r % CAP
    hit = place_of_r == pos_row
    for q in range(QUART):
        place[:, q * tokens:(q + 1) * tokens] = onehot(hit & ((r // CAP) % QUART == q))
    msgs[...] = jnp.dot(place[...], stack[...], preferred_element_type=F32).astype(BF16).reshape(SLOTS, BLOCK, part)
    xbuf[0, 0] = msgs[0]

    line = iota((128, tokens), 0)
    of_line = (jnp.where(first % 4 == line % 4, gw_ref[0:1, :], 0.0)
               + jnp.where(second % 4 == line % 4, gw_ref[1:2, :], 0.0))
    of_line = jnp.where(rank == line // 4, of_line, 0.0)
    chosen = jnp.where(iota((SLOTS, tokens), 0) == slot_row, 1.0, 0.0)
    meta = lax.dot_general(chosen, of_line, (((1,), (1,)), ((), ())), preferred_element_type=F32, precision=HIGHEST)
    for slot in range(SLOTS):
        meta_out[0, slot] = meta[slot:slot + 1, :]

    with jax.named_scope("barrier"):
        pl.semaphore_wait(barrier, SLOTS + 2 + 2 * len(near))

    def remote(src, dst, send, recv, device):
        return pltpu.make_async_remote_copy(src_ref=src, dst_ref=dst, send_sem=send, recv_sem=recv,
                                            device_id=device, device_id_type=MESH)

    sides = (right, {"tp": (mx + 2) % 4}, left)
    for n, side in enumerate(sides):
        remote(meta_out.at[0], meta_out.at[n + 1], xm_send.at[n], xm_recv.at[n], side).start()

    def span(name, kind):
        first_slot, count = START[name], COUNT[name]
        low, high = {None: (0, count), AGA: (0, count // 2), AGB: (count // 2, count)}[kind]
        return slice(first_slot + low, first_slot + high)

    def send_over(name):
        for slot in slots_of(name):
            if slot:
                n = NAMES.index(name)
                remote(msgs.at[slot], xbuf.at[0, slot], y_send, y_recv.at[n], peer(slot, -1)).start()

    def send_direct(name):
        n = NAMES.index(name)
        at, count = START[name], COUNT[name]
        for step in range(count):
            for side, held, slot in ((RIGHT, 1, at + step), (LEFT, 3, at + (step + count // 2) % count)):
                kind = AGA if slot < at + count // 2 else AGB
                remote(msgs.at[slot], xbuf.at[held, slot], x_send.at[side], x_recv.at[side, kind, n],
                       peer(slot, -1, -1 if side else 1)).start()
        send_over(name)

    def constants():
        for size, spread, gather in zip(SIZES, spreads, gathers):
            edge = 2 * size * BLOCK
            run = 2 * size * CAP
            a, b = iota((edge, edge), 0), iota((edge, edge), 1)
            spread[...] = onehot(((a % run) // CAP) * BLOCK + (a // run) * CAP + a % CAP == b)
            gather[...] = onehot(((b % run) // CAP) * BLOCK + (b // run) * CAP + b % CAP == a)
        r = iota((tokens, SLOTS * BLOCK), 1)
        hit = (r // BLOCK) * CAP + r % CAP == pos_col
        for q in range(QUART):
            unplace[q * tokens:(q + 1) * tokens, :] = onehot(hit & ((r // CAP) % QUART == q))

    def hop(side, src, dst, kind, name):
        return remote(src, dst, x_send.at[side], x_recv.at[side, kind, NAMES.index(name)], left if side else right)

    def ag(side, kind, name):
        part_of = span(name, kind)
        return hop(side, xbuf.at[0, part_of], xbuf.at[3 if side else 1, part_of], kind, name)

    def fwd(side, name):
        part_of = span(name, side)
        return hop(side, xbuf.at[3 if side else 1, part_of], xbuf.at[2, part_of], FWD, name)

    def rs_first(side, name):
        part_of = span(name, side)
        return hop(side, cbuf.at[2, part_of], rs1.at[part_of], RS1, name)

    def rs_second(side, kind, name):
        part_of = span(name, kind - RS2A)
        return hop(side, cbuf.at[1 if side else 3, part_of], rs2.at[side, part_of], kind, name)

    def over_done(name):
        first_slot = max(1, START[name])
        src = xbuf.at[0, slice(first_slot, START[name] + COUNT[name])]
        remote(src, src, y_send, y_recv.at[NAMES.index(name)], right).wait_recv()

    def start_gather(name):
        over_done(name)
        ag(RIGHT, AGA, name).start()
        ag(LEFT, AGB, name).start()
        ag(RIGHT, AGB, name).start()
        ag(LEFT, AGA, name).start()

    def forward(name):
        ag(RIGHT, AGA, name).wait_recv()
        fwd(RIGHT, name).start()
        ag(LEFT, AGB, name).wait_recv()
        fwd(LEFT, name).start()

    def meta_send():
        for n, side in enumerate(sides):
            remote(meta_out.at[0], meta_out.at[n + 1], xm_send.at[n], xm_recv.at[n], side).wait_recv()
        for slot in range(1, SLOTS):
            remote(meta_out.at[:, slot], xmeta.at[:, slot], m_send, m_recv, peer(slot, -1)).start()

    def meta_use():
        src = xmeta.at[:, slice(1, SLOTS)]
        remote(src, src, m_send, m_recv, right).wait_recv()
        for side in range(4):
            for slot in range(SLOTS):
                row = xmeta[side, slot] if slot else meta_out[side, 0]
                mrows[side * SLOTS + slot:side * SLOTS + slot + 1, :] = row
        for name in NAMES:
            at, count = START[name], COUNT[name]
            n, col = iota((count * BLOCK, 4 * SLOTS), 0), iota((count * BLOCK, 4 * SLOTS), 1)
            source = (n // (count * CAP)) * SLOTS + at + (n % (count * CAP)) // CAP
            picked = jnp.dot(jnp.where(source == col, 1.0, 0.0), mrows[...], preferred_element_type=F32, precision=HIGHEST)
            mine = (n % CAP) * 4 + mx == col
            gall[at * BLOCK:(at + count) * BLOCK, :] = jnp.broadcast_to(
                jnp.sum(jnp.where(mine, picked, 0.0), axis=1, keepdims=True), (count * BLOCK, 128))

    started = []

    def compute(name):
        at, count = START[name], COUNT[name]
        spread, gather = spreads[SIZES.index(count)], gathers[SIZES.index(count)]
        edge, run, total_rows = 2 * count * BLOCK, 2 * count * CAP, 4 * count * CAP
        if name in DIRECT:
            over_done(name)
        ag(RIGHT, AGB, name).wait_recv()
        ag(LEFT, AGA, name).wait_recv()
        fwd(RIGHT, name).wait_recv()
        fwd(LEFT, name).wait_recv()
        for pair in range(2):
            block = xbuf[2 * pair:2 * pair + 2, span(name, None)].reshape(edge, part)
            ordered = jnp.dot(spread[...], block, preferred_element_type=F32).astype(BF16)
            for q in range(QUART):
                rows[pair * run:(pair + 1) * run, q * part:(q + 1) * part] = ordered[q * run:(q + 1) * run]
        if not started:
            weights[0].wait()
            weights[1].wait()
        inputs = rows[0:total_rows, :]
        gate = jnp.dot(inputs, wg[...], preferred_element_type=F32)
        up = jnp.dot(inputs, wu[...], preferred_element_type=F32)
        hidden = (gate / (1.0 + jnp.exp(-gate)) * up).astype(BF16)
        if not started:
            weights[2].wait()
            started.append(name)
        weight = gall[at * BLOCK:(at + count) * BLOCK, 0:1]
        for q in range(QUART):
            piece_out = jnp.dot(hidden, wd[:, q * part:(q + 1) * part], preferred_element_type=F32)
            piece_out = (piece_out * weight).astype(BF16)
            for pair in range(2):
                ybuf[pair * edge + q * run:pair * edge + (q + 1) * run, :] = piece_out[pair * run:(pair + 1) * run]
        for pair in (1, 0):
            block = jnp.dot(gather[...], ybuf[pair * edge:(pair + 1) * edge, :], preferred_element_type=F32).astype(BF16)
            cbuf[2 * pair:2 * pair + 2, span(name, None)] = block.reshape(2, count, BLOCK, part)
            if pair == 1:
                rs_first(RIGHT, name).start()
                rs_first(LEFT, name).start()
        rs_second(RIGHT, RS2B, name).start()
        rs_second(LEFT, RS2A, name).start()

    def reduce_first(name):
        for side, held, kind in ((RIGHT, 3, RS2A), (LEFT, 1, RS2B)):
            rs_first(side, name).wait_recv()
            mine = span(name, side)
            cbuf[held, mine] = (cbuf[held, mine].astype(F32) + rs1[mine].astype(F32)).astype(BF16)
            rs_second(side, kind, name).start()

    def give_back(name):
        for side in (RIGHT, LEFT):
            rs_second(side, RS2A, name).wait_recv()
            rs_second(side, RS2B, name).wait_recv()
        all_of = span(name, None)
        total = cbuf[0, all_of].astype(F32) + rs2[RIGHT, all_of].astype(F32) + rs2[LEFT, all_of].astype(F32)
        back[all_of] = total.astype(BF16)
        for slot in slots_of(name):
            if slot:
                remote(back.at[slot], ret.at[slot], b_send, b_recv, peer(slot, 1)).start()
            else:
                ret[0] = back[0]

    steps = {"d": send_direct, "g": start_gather, "f": forward, "c": compute, "r": reduce_first, "b": give_back, "o": send_over}
    plain = {"k": constants, "mS": meta_send, "mU": meta_use}
    for what in ORDER:
        with jax.named_scope(what):
            plain[what]() if what in plain else steps[what[0]](what[1])

    with jax.named_scope("sent"):
        src = msgs.at[slice(1, SLOTS)]
        remote(src, src, y_send, y_recv.at[0], right).wait_send()
        for side in (RIGHT, LEFT):
            src = xbuf.at[slice(0, 3)]
            remote(src, src, x_send.at[side], x_recv.at[0, 0, 0], right).wait_send()
        src = meta_out.at[:, slice(1, SLOTS)]
        remote(src, src, m_send, m_recv, right).wait_send()
        for n in range(3):
            remote(meta_out.at[0], meta_out.at[1], xm_send.at[n], xm_recv.at[n], right).wait_send()
    with jax.named_scope("back"):
        src = ret.at[slice(1, SLOTS)]
        remote(src, src, b_send, b_recv, right).wait_recv()
    with jax.named_scope("final"):
        result = jnp.dot(unplace[...], ret[...].reshape(SLOTS * BLOCK, part), preferred_element_type=F32).astype(BF16)
        for q in range(QUART):
            out_ref[:, q * part:(q + 1) * part] = result[q * tokens:(q + 1) * tokens]
        remote(src, src, b_send, b_recv, right).wait_send()


def local(tokens, norm_gain, w_gate, w_up, w_down, routing, gate_weight):
    count, width = tokens.shape
    hidden = w_gate.shape[2]
    part = width // QUART
    total = SLOTS * BLOCK
    vmem = pl.BlockSpec(memory_space=pltpu.VMEM)
    hbm = pl.BlockSpec(memory_space=pltpu.HBM)
    dma = pltpu.SemaphoreType.DMA
    return pl.pallas_call(
        kernel,
        out_shape=jax.ShapeDtypeStruct((count, width), BF16),
        in_specs=[hbm] * 7,
        out_specs=vmem,
        scratch_shapes=[
            pltpu.VMEM((count, width), BF16),
            pltpu.VMEM((1, width), F32),
            pltpu.VMEM((2, count), I32),
            pltpu.VMEM((2, count), F32),
            pltpu.VMEM((width, hidden), BF16),
            pltpu.VMEM((width, hidden), BF16),
            pltpu.VMEM((hidden, width), BF16),
            pltpu.VMEM((QUART * count, part), BF16),
            pltpu.VMEM((total, QUART * count), BF16),
            pltpu.VMEM((QUART * count, total), BF16),
            [pltpu.VMEM((2 * size * BLOCK, 2 * size * BLOCK), BF16) for size in SIZES],
            [pltpu.VMEM((2 * size * BLOCK, 2 * size * BLOCK), BF16) for size in SIZES],
            pltpu.VMEM((SLOTS, BLOCK, part), BF16),
            pltpu.VMEM((4, SLOTS, 1, 128), F32),
            pltpu.VMEM((4, SLOTS, BLOCK, part), BF16),
            pltpu.VMEM((4, SLOTS, 1, 128), F32),
            pltpu.VMEM((4 * SLOTS, 128), F32),
            pltpu.VMEM((4 * SLOTS * CAP, 128), F32),
            pltpu.VMEM((max(SIZES) * BLOCK, width), BF16),
            pltpu.VMEM((4 * max(SIZES) * BLOCK, part), BF16),
            pltpu.VMEM((4, SLOTS, BLOCK, part), BF16),
            pltpu.VMEM((SLOTS, BLOCK, part), BF16),
            pltpu.VMEM((2, SLOTS, BLOCK, part), BF16),
            pltpu.VMEM((SLOTS, BLOCK, part), BF16),
            pltpu.VMEM((SLOTS, BLOCK, part), BF16),
            dma((7,)), dma, dma((len(NAMES),)), dma, dma,
            dma((2,)), dma((2, 6, len(NAMES))), dma((3,)), dma((3,)), dma, dma,
        ],
        compiler_params=pltpu.CompilerParams(
            collective_id=0, has_side_effects=True, vmem_limit_bytes=54 * 1024 * 1024
        ),
    )(tokens, norm_gain.reshape(1, width), w_gate, w_up, w_down, routing.T, gate_weight.T)


def solution(mesh):
    placed = (
        P(("ep", "tp"), None),
        P(),
        P(("ep", "tp"), None, None),
        P(("ep", "tp"), None, None),
        P(("ep", "tp"), None, None),
        P(("ep", "tp"), None),
        P(("ep", "tp"), None),
    )
    return jax.shard_map(
        local, mesh=mesh, in_specs=placed, out_specs=P(("ep", "tp"), None), check_vma=False
    )
```

```python
import functools

import jax
import jax.numpy as jnp
from jax import lax
from jax.experimental import pallas as pl
from jax.experimental.pallas import tpu as pltpu
from jax.sharding import PartitionSpec as P

MESH = pl.DeviceIdType.MESH
F32, BF16, I32 = jnp.float32, jnp.bfloat16, jnp.int32
HIGHEST = lax.Precision.HIGHEST

CHUNKS = {
    "E": ((0, 0),),
    "A": ((0, 1), (0, 3), (1, 0), (3, 0)),
    "B": ((2, 0), (2, 1), (0, 2), (1, 2)),
    "D": ((1, 1), (3, 3), (1, 3)),
    "C": ((2, 2), (2, 3), (3, 2), (3, 1)),
}
NAMES = tuple(CHUNKS)
DIRECT = "EA"
PAIRS = tuple(pair for name in NAMES for pair in CHUNKS[name])
SLOTS = 2 * len(PAIRS)
COUNT = {name: 2 * len(CHUNKS[name]) for name in NAMES}
START = {name: 2 * PAIRS.index(CHUNKS[name][0]) for name in NAMES}
CAP = 4
QUART = 4
BLOCK = CAP * QUART
AGA, AGB, FWD, RS1, RS2A, RS2B = range(6)
RIGHT, LEFT = 0, 1
PIECES = 1
NEAR = sum(COUNT[name] for name in DIRECT)
SIZES = tuple(sorted(set(COUNT.values())))
ORDER = (
    "dE", "oD", "dA", "oC", "oB", "k", "fE", "gD", "fA", "mS", "gC", "fD", "gB", "fC", "mU", "cD",
    "fB", "cC", "cB", "rC", "rD", "rB", "cA", "bC", "cE", "bD", "bB", "rA", "rE",
)


def iota(shape, dim):
    return lax.broadcasted_iota(I32, shape, dim)


def onehot(mask):
    return jnp.where(mask, 1.0, 0.0).astype(BF16)


def here():
    me = lax.axis_index("ep")
    return me // 8, (me // 2) % 4, me % 2


def slots_and_ranks(route_ref, tokens):
    z, y, c = here()
    group = route_ref[0:1, :] // 4
    square = jnp.broadcast_to(group.astype(F32), (tokens, tokens))
    earlier = (square.T == square) & (iota((tokens, tokens), 0) < iota((tokens, tokens), 1))
    rank = jnp.sum(jnp.where(earlier, 1, 0), axis=0, keepdims=True)
    rel = ((z + 4 - group // 8) % 4) * 4 + (y + 4 - (group // 2) % 4) % 4
    pair = jnp.zeros_like(group)
    for n, (dz, dy) in enumerate(PAIRS):
        pair = pair + jnp.where(rel == dz * 4 + dy, n, 0)
    return pair * 2 + (group + c) % 2, rank


def kernel(tok_hbm, gain_hbm, wg_hbm, wu_hbm, wd_hbm, route_hbm, gw_hbm, ret,
           tok_ref, gain_ref, route_ref, gw_ref, wg, wu, wd, stack, place, spreads, gathers, msgs, meta_out, xbuf, xmeta, mrows, gall,
           rows, ybuf, cbuf, rs1, rs2, back,
           w_sem, y_send, y_recv, m_send, m_recv, x_send, x_recv, xm_send, xm_recv, b_send, b_recv, p_recv, own_sem):
    tokens, width = tok_ref.shape
    part = width // QUART
    mx = lax.axis_index("tp")
    z, y, c = here()
    right = {"tp": (mx + 1) % 4}
    left = {"tp": (mx + 3) % 4}

    def peer(slot, sign, dx=0):
        dz, dy = PAIRS[slot // 2]
        dc = slot % 2
        group = ((z + 4 + sign * dz) % 4) * 8 + ((y + 4 + sign * dy) % 4) * 2 + (c + dc) % 2
        return {"ep": group, "tp": (mx + 4 + dx) % 4}

    def slots_of(name):
        return range(START[name], START[name] + COUNT[name])

    small = [pltpu.make_async_copy(src, dst, w_sem.at[3 + n]) for n, (src, dst) in enumerate((
        (tok_hbm, tok_ref), (gain_hbm, gain_ref), (route_hbm, route_ref), (gw_hbm, gw_ref)))]
    for copy in small:
        copy.start()
    weights = [pltpu.make_async_copy(src.at[0], dst, w_sem.at[n])
               for n, (src, dst) in enumerate(((wg_hbm, wg), (wu_hbm, wu), (wd_hbm, wd)))]

    barrier = pltpu.get_barrier_semaphore()
    for slot in range(1, SLOTS):
        pl.semaphore_signal(barrier, inc=1, device_id=peer(slot, -1), device_id_type=MESH)
    near = [slot for name in DIRECT for slot in slots_of(name) if slot]
    for slot in near:
        for dx in (1, -1):
            pl.semaphore_signal(barrier, inc=1, device_id=peer(slot, -1, dx), device_id_type=MESH)
    for side in (right, {"tp": (mx + 2) % 4}, left):
        pl.semaphore_signal(barrier, inc=1, device_id=side, device_id_type=MESH)

    for copy in small:
        copy.wait()
    for copy in weights:
        copy.start()
    values = tok_ref[...].astype(F32)
    scale = lax.rsqrt(jnp.mean(values * values, axis=-1, keepdims=True) + 1e-06)
    normed = (values * scale * gain_ref[...]).astype(BF16)
    for q in range(QUART):
        stack[q * tokens:(q + 1) * tokens, :] = normed[:, q * part:(q + 1) * part]

    slot_row, rank = slots_and_ranks(route_ref, tokens)
    pos_row = slot_row * CAP + rank

    r = iota((SLOTS * BLOCK, tokens), 0)
    place_of_r = (r // BLOCK) * CAP + r % CAP
    hit = place_of_r == pos_row
    for q in range(QUART):
        place[:, q * tokens:(q + 1) * tokens] = onehot(hit & ((r // CAP) % QUART == q))
    msgs[...] = jnp.dot(place[...], stack[...], preferred_element_type=F32).astype(BF16).reshape(SLOTS, BLOCK, part)
    xbuf[0, 0] = msgs[0]

    first, second = route_ref[0:1, :], route_ref[1:2, :]
    line = iota((128, tokens), 0)
    of_line = (jnp.where(first % 4 == line % 4, gw_ref[0:1, :], 0.0)
               + jnp.where(second % 4 == line % 4, gw_ref[1:2, :], 0.0))
    of_line = jnp.where((slot_row % 8) * CAP + rank == line // 4, of_line, 0.0)
    chosen = jnp.where(iota((8, tokens), 0) == slot_row // 8, 1.0, 0.0)
    meta = lax.dot_general(chosen, of_line, (((1,), (1,)), ((), ())), preferred_element_type=F32, precision=HIGHEST)
    for n in range(SLOTS // 8):
        meta_out[0, n] = meta[n:n + 1, :]

    with jax.named_scope("barrier"):
        pl.semaphore_wait(barrier, SLOTS + 2 + 2 * len(near))

    def remote(src, dst, send, recv, device):
        return pltpu.make_async_remote_copy(src_ref=src, dst_ref=dst, send_sem=send, recv_sem=recv,
                                            device_id=device, device_id_type=MESH)

    sides = (right, {"tp": (mx + 2) % 4}, left)
    for n, side in enumerate(sides):
        remote(meta_out.at[0], meta_out.at[n + 1], xm_send.at[n], xm_recv.at[n], side).start()

    def span(name, kind):
        first_slot, count = START[name], COUNT[name]
        low, high = {None: (0, count), AGA: (0, count // 2), AGB: (count // 2, count)}[kind]
        return slice(first_slot + low, first_slot + high)

    def send_over(name):
        for slot in slots_of(name):
            if slot:
                n, upper = NAMES.index(name), int(slot >= START[name] + COUNT[name] // 2)
                remote(msgs.at[slot], xbuf.at[0, slot], y_send, y_recv.at[upper, n], peer(slot, -1)).start()

    def send_direct(name):
        n = NAMES.index(name)
        at, count = START[name], COUNT[name]
        for step in range(count):
            for side, held, slot in ((RIGHT, 1, at + step), (LEFT, 3, at + (step + count // 2) % count)):
                kind = AGA if slot < at + count // 2 else AGB
                remote(msgs.at[slot], xbuf.at[held, slot], x_send.at[side], x_recv.at[side, kind, n],
                       peer(slot, -1, -1 if side else 1)).start()
        send_over(name)

    def constants():
        for size, spread, gather in zip(SIZES, spreads, gathers):
            edge = 2 * size * BLOCK
            run = 2 * size * CAP
            a, b = iota((edge, edge), 0), iota((edge, edge), 1)
            spread[...] = onehot(((a % run) // CAP) * BLOCK + (a // run) * CAP + a % CAP == b)
            gather[...] = onehot(((b % run) // CAP) * BLOCK + (b // run) * CAP + b % CAP == a)

    def hop(side, src, dst, kind, name):
        return remote(src, dst, x_send.at[side], x_recv.at[side, kind, NAMES.index(name)], left if side else right)

    def ag(side, kind, name):
        part_of = span(name, kind)
        return hop(side, xbuf.at[0, part_of], xbuf.at[3 if side else 1, part_of], kind, name)

    def fwd(side, name):
        part_of = span(name, side)
        return hop(side, xbuf.at[3 if side else 1, part_of], xbuf.at[2, part_of], FWD, name)

    def rs_first(side, name):
        part_of = span(name, side)
        return hop(side, cbuf.at[2, part_of], rs1.at[part_of], RS1, name)

    def rs_second(side, kind, name):
        part_of = span(name, kind - RS2A)
        return hop(side, cbuf.at[1 if side else 3, part_of], rs2.at[side, part_of], kind, name)

    def over_done(name, kind):
        half_of = span(name, kind)
        if half_of.stop > 1:
            src = xbuf.at[0, slice(max(1, half_of.start), half_of.stop)]
            remote(src, src, y_send, y_recv.at[kind, NAMES.index(name)], right).wait_recv()

    def start_gather(name):
        for kind in (AGA, AGB):
            over_done(name, kind)
            ag(RIGHT, kind, name).start()
            ag(LEFT, kind, name).start()

    def forward(name):
        ag(RIGHT, AGA, name).wait_recv()
        fwd(RIGHT, name).start()
        ag(LEFT, AGB, name).wait_recv()
        fwd(LEFT, name).start()

    def meta_send():
        for n, side in enumerate(sides):
            remote(meta_out.at[0], meta_out.at[n + 1], xm_send.at[n], xm_recv.at[n], side).wait_recv()
        for slot in range(1, SLOTS):
            remote(meta_out.at[:, slot // 8], xmeta.at[:, slot], m_send, m_recv, peer(slot, -1)).start()

    def meta_use():
        src = xmeta.at[:, slice(1, SLOTS)]
        remote(src, src, m_send, m_recv, right).wait_recv()
        for side in range(4):
            for slot in range(SLOTS):
                row = xmeta[side, slot] if slot else meta_out[side, 0]
                mrows[side * SLOTS + slot:side * SLOTS + slot + 1, :] = row
        for name in NAMES:
            at, count = START[name], COUNT[name]
            n, col = iota((count * BLOCK, 4 * SLOTS), 0), iota((count * BLOCK, 4 * SLOTS), 1)
            source = (n // (count * CAP)) * SLOTS + at + (n % (count * CAP)) // CAP
            picked = jnp.dot(jnp.where(source == col, 1.0, 0.0), mrows[...], preferred_element_type=F32, precision=HIGHEST)
            mine = ((at + (n % (count * CAP)) // CAP) % 8) * 16 + (n % CAP) * 4 + mx == col
            gall[at * BLOCK:(at + count) * BLOCK, :] = jnp.broadcast_to(
                jnp.sum(jnp.where(mine, picked, 0.0), axis=1, keepdims=True), (count * BLOCK, 128))

    started = []

    def compute(name):
        at, count = START[name], COUNT[name]
        spread, gather = spreads[SIZES.index(count)], gathers[SIZES.index(count)]
        edge, run, total_rows = 2 * count * BLOCK, 2 * count * CAP, 4 * count * CAP
        if name in DIRECT:
            over_done(name, AGA)
            over_done(name, AGB)
        ag(RIGHT, AGB, name).wait_recv()
        ag(LEFT, AGA, name).wait_recv()
        fwd(RIGHT, name).wait_recv()
        fwd(LEFT, name).wait_recv()
        for pair in range(2):
            block = xbuf[2 * pair:2 * pair + 2, span(name, None)].reshape(edge, part)
            ordered = jnp.dot(spread[...], block, preferred_element_type=F32).astype(BF16)
            for q in range(QUART):
                rows[pair * run:(pair + 1) * run, q * part:(q + 1) * part] = ordered[q * run:(q + 1) * run]
        if not started:
            weights[0].wait()
            weights[1].wait()
        inputs = rows[0:total_rows, :]
        gate = jnp.dot(inputs, wg[...], preferred_element_type=F32)
        up = jnp.dot(inputs, wu[...], preferred_element_type=F32)
        hidden = (gate / (1.0 + jnp.exp(-gate)) * up).astype(BF16)
        if not started:
            weights[2].wait()
            started.append(name)
        weight = gall[at * BLOCK:(at + count) * BLOCK, 0:1]
        for q in range(QUART):
            piece_out = jnp.dot(hidden, wd[:, q * part:(q + 1) * part], preferred_element_type=F32)
            piece_out = (piece_out * weight).astype(BF16)
            for pair in range(2):
                ybuf[pair * edge + q * run:pair * edge + (q + 1) * run, :] = piece_out[pair * run:(pair + 1) * run]
        for pair in (1, 0):
            block = jnp.dot(gather[...], ybuf[pair * edge:(pair + 1) * edge, :], preferred_element_type=F32).astype(BF16)
            cbuf[2 * pair:2 * pair + 2, span(name, None)] = block.reshape(2, count, BLOCK, part)
            if pair == 1:
                rs_first(RIGHT, name).start()
                rs_first(LEFT, name).start()
        if name in DIRECT:
            to_source(name, RIGHT, AGB)
            to_source(name, LEFT, AGA)
            for slot in slots_of(name):
                if slot:
                    remote(cbuf.at[0, slot], ret.at[slot], b_send, b_recv, peer(slot, 1)).start()
                else:
                    pltpu.make_async_copy(cbuf.at[0, slot], ret.at[slot], own_sem).start()
        else:
            rs_second(RIGHT, RS2B, name).start()
            rs_second(LEFT, RS2A, name).start()

    def to_source(name, side, kind):
        half_of = span(name, kind)
        for slot in range(half_of.start, half_of.stop):
            remote(cbuf.at[1 if side else 3, slot], ret.at[SLOTS + side * NEAR + slot], x_send.at[side], p_recv,
                   peer(slot, 1, -1 if side else 1)).start()

    def reduce_first(name):
        for side, held, kind in ((RIGHT, 3, RS2A), (LEFT, 1, RS2B)):
            rs_first(side, name).wait_recv()
            mine = span(name, side)
            cbuf[held, mine] = (cbuf[held, mine].astype(F32) + rs1[mine].astype(F32)).astype(BF16)
            if name in DIRECT:
                to_source(name, side, side)
            else:
                rs_second(side, kind, name).start()

    def give_back(name):
        for side in (RIGHT, LEFT):
            rs_second(side, RS2A, name).wait_recv()
            rs_second(side, RS2B, name).wait_recv()
        all_of = span(name, None)
        total = cbuf[0, all_of].astype(F32) + rs2[RIGHT, all_of].astype(F32) + rs2[LEFT, all_of].astype(F32)
        back[all_of] = total.astype(BF16)
        for slot in slots_of(name):
            remote(back.at[slot], ret.at[slot], b_send, b_recv, peer(slot, 1)).start()

    steps = {"d": send_direct, "g": start_gather, "f": forward, "c": compute, "r": reduce_first, "b": give_back, "o": send_over}
    plain = {"k": constants, "mS": meta_send, "mU": meta_use}
    for what in ORDER:
        with jax.named_scope(what):
            plain[what]() if what in plain else steps[what[0]](what[1])

    with jax.named_scope("sent"):
        src = msgs.at[slice(1, SLOTS)]
        remote(src, src, y_send, y_recv.at[0, 0], right).wait_send()
        for side in (RIGHT, LEFT):
            src = xbuf.at[slice(0, 3)]
            remote(src, src, x_send.at[side], x_recv.at[0, 0, 0], right).wait_send()
        src = xmeta.at[:, slice(1, SLOTS)]
        remote(src, src, m_send, m_recv, right).wait_send()
        for n in range(3):
            remote(meta_out.at[0], meta_out.at[1], xm_send.at[n], xm_recv.at[n], right).wait_send()
    with jax.named_scope("back"):
        src = ret.at[slice(1, SLOTS)]
        remote(src, src, b_send, b_recv, right).wait_recv()
        src = ret.at[slice(SLOTS, SLOTS + 2 * NEAR)]
        remote(src, src, b_send, p_recv, right).wait_recv()
        pltpu.make_async_copy(cbuf.at[0, 0], ret.at[0], own_sem).wait()
        src = xbuf.at[0, slice(1, SLOTS)]
        remote(src, src, b_send, b_recv, right).wait_send()


def finish(ret_hbm, route_hbm, out_hbm, ret, route_ref, unplace, out, in_sem, out_sem):
    tokens = route_ref.shape[1]
    part = ret.shape[2]
    piece = part // PIECES
    fetch = [pltpu.make_async_copy(route_hbm, route_ref, in_sem.at[PIECES])]
    for n in range(PIECES):
        columns = slice(n * piece, (n + 1) * piece)
        fetch.append(pltpu.make_async_copy(ret_hbm.at[:, :, columns], ret.at[:, :, columns], in_sem.at[n]))
    for copy in fetch:
        copy.start()
    fetch[0].wait()
    slot_row, rank = slots_and_ranks(route_ref, tokens)
    pos_col = jnp.broadcast_to((slot_row * CAP + rank).astype(F32), (tokens, tokens)).T[:, 0:1].astype(I32)
    r = iota((tokens, SLOTS * BLOCK), 1)
    hit = (r // BLOCK) * CAP + r % CAP == pos_col
    for q in range(QUART):
        unplace[q * tokens:(q + 1) * tokens, :] = onehot(hit & ((r // CAP) % QUART == q))
    copies = []
    for n in range(PIECES):
        fetch[1 + n].wait()
        columns = slice(n * piece, (n + 1) * piece)
        near, near_left = slice(SLOTS, SLOTS + NEAR), slice(SLOTS + NEAR, SLOTS + 2 * NEAR)
        total = (ret[0:NEAR, :, columns].astype(F32) + ret[near, :, columns].astype(F32)
                 + ret[near_left, :, columns].astype(F32))
        stacked = jnp.concatenate([total.astype(BF16), ret[NEAR:SLOTS, :, columns]], axis=0)
        row = jnp.dot(unplace[...], stacked.reshape(SLOTS * BLOCK, piece), preferred_element_type=F32).astype(BF16)
        for q in range(QUART):
            to = slice(q * part + n * piece, q * part + (n + 1) * piece)
            out[:, to] = row[q * tokens:(q + 1) * tokens]
            copies.append(pltpu.make_async_copy(out.at[:, to], out_hbm.at[:, to], out_sem.at[n, q]))
            copies[-1].start()
    for copy in copies:
        copy.wait()


def local(tokens, norm_gain, w_gate, w_up, w_down, routing, gate_weight):
    count, width = tokens.shape
    hidden = w_gate.shape[2]
    part = width // QUART
    total = SLOTS * BLOCK
    hbm = pl.BlockSpec(memory_space=pltpu.HBM)
    dma = pltpu.SemaphoreType.DMA
    returned = pl.pallas_call(
        kernel,
        out_shape=jax.ShapeDtypeStruct((SLOTS + 2 * NEAR, BLOCK, part), BF16),
        in_specs=[hbm] * 7,
        out_specs=hbm,
        scratch_shapes=[
            pltpu.VMEM((count, width), BF16),
            pltpu.VMEM((1, width), F32),
            pltpu.VMEM((2, count), I32),
            pltpu.VMEM((2, count), F32),
            pltpu.VMEM((width, hidden), BF16),
            pltpu.VMEM((width, hidden), BF16),
            pltpu.VMEM((hidden, width), BF16),
            pltpu.VMEM((QUART * count, part), BF16),
            pltpu.VMEM((total, QUART * count), BF16),
            [pltpu.VMEM((2 * size * BLOCK, 2 * size * BLOCK), BF16) for size in SIZES],
            [pltpu.VMEM((2 * size * BLOCK, 2 * size * BLOCK), BF16) for size in SIZES],
            pltpu.VMEM((SLOTS, BLOCK, part), BF16),
            pltpu.VMEM((4, SLOTS // 8, 1, 128), F32),
            pltpu.VMEM((4, SLOTS, BLOCK, part), BF16),
            pltpu.VMEM((4, SLOTS, 1, 128), F32),
            pltpu.VMEM((4 * SLOTS, 128), F32),
            pltpu.VMEM((4 * SLOTS * CAP, 128), F32),
            pltpu.VMEM((max(SIZES) * BLOCK, width), BF16),
            pltpu.VMEM((4 * max(SIZES) * BLOCK, part), BF16),
            pltpu.VMEM((4, SLOTS, BLOCK, part), BF16),
            pltpu.VMEM((SLOTS, BLOCK, part), BF16),
            pltpu.VMEM((2, SLOTS, BLOCK, part), BF16),
            pltpu.VMEM((SLOTS, BLOCK, part), BF16),
            dma((7,)), dma, dma((2, len(NAMES))), dma, dma,
            dma((2,)), dma((2, 6, len(NAMES))), dma((3,)), dma((3,)), dma, dma, dma, dma,
        ],
        compiler_params=pltpu.CompilerParams(
            collective_id=0, has_side_effects=True, vmem_limit_bytes=54 * 1024 * 1024
        ),
    )(tokens, norm_gain.reshape(1, width), w_gate, w_up, w_down, routing.T, gate_weight.T)
    return pl.pallas_call(
        finish,
        out_shape=jax.ShapeDtypeStruct((count, width), BF16),
        in_specs=[hbm] * 2,
        out_specs=hbm,
        scratch_shapes=[
            pltpu.VMEM((SLOTS + 2 * NEAR, BLOCK, part), BF16),
            pltpu.VMEM((2, count), I32),
            pltpu.VMEM((QUART * count, total), BF16),
            pltpu.VMEM((count, width), BF16),
            dma((PIECES + 1,)), dma((PIECES, QUART)),
        ],
        compiler_params=pltpu.CompilerParams(vmem_limit_bytes=54 * 1024 * 1024),
    )(returned, routing.T)


def solution(mesh):
    placed = (
        P(("ep", "tp"), None),
        P(),
        P(("ep", "tp"), None, None),
        P(("ep", "tp"), None, None),
        P(("ep", "tp"), None, None),
        P(("ep", "tp"), None),
        P(("ep", "tp"), None),
    )
    return jax.shard_map(
        local, mesh=mesh, in_specs=placed, out_specs=P(("ep", "tp"), None), check_vma=False
    )
```

```python
import functools

import jax
import jax.numpy as jnp
from jax import lax
from jax.experimental import pallas as pl
from jax.experimental.pallas import tpu as pltpu
from jax.sharding import PartitionSpec as P

MESH = pl.DeviceIdType.MESH
F32, BF16, I32 = jnp.float32, jnp.bfloat16, jnp.int32
HIGHEST = lax.Precision.HIGHEST

CHUNKS = {
    "E": ((0, 0),),
    "A": ((0, 1), (0, 3), (1, 0), (3, 0)),
    "D": ((1, 1), (3, 3), (1, 3)),
    "B": ((2, 0), (2, 1), (0, 2), (1, 2)),
    "C": ((2, 2), (2, 3), (3, 2), (3, 1)),
}
NAMES = tuple(CHUNKS)
DIRECT = "EA"
PAIRS = tuple(pair for name in NAMES for pair in CHUNKS[name])
SLOTS = 2 * len(PAIRS)
COUNT = {name: 2 * len(CHUNKS[name]) for name in NAMES}
START = {name: 2 * PAIRS.index(CHUNKS[name][0]) for name in NAMES}
CAP = 4
QUART = 4
BLOCK = CAP * QUART
AGA, AGB, FWD, RS1, RS2A, RS2B = range(6)
RIGHT, LEFT = 0, 1
PIECES = 1
NEAR = sum(COUNT[name] for name in DIRECT)
EARLY = START["B"]
SIZES = tuple(sorted(set(COUNT.values())))
ORDER = (
    "dE", "oD", "dA", "oC", "oB", "m", "k", "fE", "gD", "fA", "mS", "gC", "fD", "gB", "fC", "mU",
    "cD", "fB", "cC", "cB", "rC", "rD", "rB", "cA", "bC", "cE", "bD", "bB", "rA", "rE",
)


def iota(shape, dim):
    return lax.broadcasted_iota(I32, shape, dim)


def onehot(mask):
    return jnp.where(mask, 1.0, 0.0).astype(BF16)


def here():
    me = lax.axis_index("ep")
    return me // 8, (me // 2) % 4, me % 2


def slots_and_ranks(route_ref, tokens):
    z, y, c = here()
    group = route_ref[0:1, :] // 4
    square = jnp.broadcast_to(group.astype(F32), (tokens, tokens))
    earlier = (square.T == square) & (iota((tokens, tokens), 0) < iota((tokens, tokens), 1))
    rank = jnp.sum(jnp.where(earlier, 1, 0), axis=0, keepdims=True)
    rel = ((z + 4 - group // 8) % 4) * 4 + (y + 4 - (group // 2) % 4) % 4
    pair = jnp.zeros_like(group)
    for n, (dz, dy) in enumerate(PAIRS):
        pair = pair + jnp.where(rel == dz * 4 + dy, n, 0)
    return pair * 2 + (group + c) % 2, rank


def kernel(tok_hbm, gain_hbm, wg_hbm, wu_hbm, wd_hbm, route_hbm, gw_hbm, ret,
           tok_ref, gain_ref, route_ref, gw_ref, wg, wu, wd, stack, place, spreads, gathers, msgs, meta_out, xbuf, xmeta, mrows, gall,
           rows, ybuf, cbuf, rs1, rs2, back,
           w_sem, y_send, y_recv, m_send, m_recv, x_send, x_recv, xm_send, xm_recv, b_send, b_recv, p_recv, own_sem):
    tokens, width = tok_ref.shape
    part = width // QUART
    mx = lax.axis_index("tp")
    z, y, c = here()
    right = {"tp": (mx + 1) % 4}
    left = {"tp": (mx + 3) % 4}

    def peer(slot, sign, dx=0):
        dz, dy = PAIRS[slot // 2]
        dc = slot % 2
        group = ((z + 4 + sign * dz) % 4) * 8 + ((y + 4 + sign * dy) % 4) * 2 + (c + dc) % 2
        return {"ep": group, "tp": (mx + 4 + dx) % 4}

    def slots_of(name):
        return range(START[name], START[name] + COUNT[name])

    small = [pltpu.make_async_copy(src, dst, w_sem.at[3 + n]) for n, (src, dst) in enumerate((
        (tok_hbm, tok_ref), (gain_hbm, gain_ref), (route_hbm, route_ref), (gw_hbm, gw_ref)))]
    for copy in small:
        copy.start()
    weights = [pltpu.make_async_copy(src.at[0], dst, w_sem.at[n])
               for n, (src, dst) in enumerate(((wg_hbm, wg), (wu_hbm, wu), (wd_hbm, wd)))]

    barrier = pltpu.get_barrier_semaphore()
    for slot in range(1, SLOTS):
        pl.semaphore_signal(barrier, inc=1, device_id=peer(slot, -1), device_id_type=MESH)
    near = [slot for name in DIRECT for slot in slots_of(name) if slot]
    for slot in near:
        for dx in (1, -1):
            pl.semaphore_signal(barrier, inc=1, device_id=peer(slot, -1, dx), device_id_type=MESH)
    for side in (right, {"tp": (mx + 2) % 4}, left):
        pl.semaphore_signal(barrier, inc=1, device_id=side, device_id_type=MESH)

    small[2].wait()
    slot_row, rank = slots_and_ranks(route_ref, tokens)
    pos_row = slot_row * CAP + rank

    r = iota((SLOTS * BLOCK, tokens), 0)
    hit = (r // BLOCK) * CAP + r % CAP == pos_row
    for q in range(QUART):
        place[:, q * tokens:(q + 1) * tokens] = onehot(hit & ((r // CAP) % QUART == q))

    for copy in small[:2]:
        copy.wait()
    for copy in weights:
        copy.start()
    values = tok_ref[...].astype(F32)
    scale = lax.rsqrt(jnp.mean(values * values, axis=-1, keepdims=True) + 1e-06)
    normed = (values * scale * gain_ref[...]).astype(BF16)
    for q in range(QUART):
        stack[q * tokens:(q + 1) * tokens, :] = normed[:, q * part:(q + 1) * part]

    def put_in_order(low, high):
        block = jnp.dot(place[low * BLOCK:high * BLOCK, :], stack[...], preferred_element_type=F32)
        msgs[low:high] = block.astype(BF16).reshape(high - low, BLOCK, part)

    put_in_order(0, EARLY)
    put_in_order(EARLY, SLOTS)
    xbuf[0, 0] = msgs[0]

    with jax.named_scope("barrier"):
        pl.semaphore_wait(barrier, SLOTS + 2 + 2 * len(near))

    def remote(src, dst, send, recv, device):
        return pltpu.make_async_remote_copy(src_ref=src, dst_ref=dst, send_sem=send, recv_sem=recv,
                                            device_id=device, device_id_type=MESH)

    sides = (right, {"tp": (mx + 2) % 4}, left)
    def meta_make():
        small[3].wait()
        first, second = route_ref[0:1, :], route_ref[1:2, :]
        line = iota((128, tokens), 0)
        of_line = (jnp.where(first % 4 == line % 4, gw_ref[0:1, :], 0.0)
                   + jnp.where(second % 4 == line % 4, gw_ref[1:2, :], 0.0))
        of_line = jnp.where((slot_row % 8) * CAP + rank == line // 4, of_line, 0.0)
        chosen = jnp.where(iota((8, tokens), 0) == slot_row // 8, 1.0, 0.0)
        meta = lax.dot_general(chosen, of_line, (((1,), (1,)), ((), ())), preferred_element_type=F32, precision=HIGHEST)
        for n in range(SLOTS // 8):
            meta_out[0, n] = meta[n:n + 1, :]
        for n, side in enumerate(sides):
            remote(meta_out.at[0], meta_out.at[n + 1], xm_send.at[n], xm_recv.at[n], side).start()

    def span(name, kind):
        first_slot, count = START[name], COUNT[name]
        low, high = {None: (0, count), AGA: (0, count // 2), AGB: (count // 2, count)}[kind]
        return slice(first_slot + low, first_slot + high)

    def send_over(name):
        for slot in slots_of(name):
            if slot:
                n, upper = NAMES.index(name), int(slot >= START[name] + COUNT[name] // 2)
                remote(msgs.at[slot], xbuf.at[0, slot], y_send, y_recv.at[upper, n], peer(slot, -1)).start()

    def send_direct(name):
        n = NAMES.index(name)
        at, count = START[name], COUNT[name]
        for step in range(count):
            for side, held, slot in ((RIGHT, 1, at + step), (LEFT, 3, at + (step + count // 2) % count)):
                kind = AGA if slot < at + count // 2 else AGB
                remote(msgs.at[slot], xbuf.at[held, slot], x_send.at[side], x_recv.at[side, kind, n],
                       peer(slot, -1, -1 if side else 1)).start()
        send_over(name)

    def constants():
        for size, spread, gather in zip(SIZES, spreads, gathers):
            edge = 2 * size * BLOCK
            run = 2 * size * CAP
            a, b = iota((edge, edge), 0), iota((edge, edge), 1)
            spread[...] = onehot(((a % run) // CAP) * BLOCK + (a // run) * CAP + a % CAP == b)
            gather[...] = onehot(((b % run) // CAP) * BLOCK + (b // run) * CAP + b % CAP == a)

    def hop(side, src, dst, kind, name):
        return remote(src, dst, x_send.at[side], x_recv.at[side, kind, NAMES.index(name)], left if side else right)

    def ag(side, kind, name):
        part_of = span(name, kind)
        return hop(side, xbuf.at[0, part_of], xbuf.at[3 if side else 1, part_of], kind, name)

    def fwd(side, name):
        part_of = span(name, side)
        return hop(side, xbuf.at[3 if side else 1, part_of], xbuf.at[2, part_of], FWD, name)

    def rs_first(side, name):
        part_of = span(name, side)
        return hop(side, cbuf.at[2, part_of], rs1.at[part_of], RS1, name)

    def rs_second(side, kind, name):
        part_of = span(name, kind - RS2A)
        return hop(side, cbuf.at[1 if side else 3, part_of], rs2.at[side, part_of], kind, name)

    def over_done(name, kind):
        half_of = span(name, kind)
        if half_of.stop > 1:
            src = xbuf.at[0, slice(max(1, half_of.start), half_of.stop)]
            remote(src, src, y_send, y_recv.at[kind, NAMES.index(name)], right).wait_recv()

    def start_gather(name):
        for kind in (AGA, AGB):
            over_done(name, kind)
            ag(RIGHT, kind, name).start()
            ag(LEFT, kind, name).start()

    def forward(name):
        ag(RIGHT, AGA, name).wait_recv()
        fwd(RIGHT, name).start()
        ag(LEFT, AGB, name).wait_recv()
        fwd(LEFT, name).start()

    def meta_send():
        for n, side in enumerate(sides):
            remote(meta_out.at[0], meta_out.at[n + 1], xm_send.at[n], xm_recv.at[n], side).wait_recv()
        for slot in range(1, SLOTS):
            remote(meta_out.at[:, slot // 8], xmeta.at[:, slot], m_send, m_recv, peer(slot, -1)).start()

    def meta_use():
        src = xmeta.at[:, slice(1, SLOTS)]
        remote(src, src, m_send, m_recv, right).wait_recv()
        for side in range(4):
            for slot in range(SLOTS):
                row = xmeta[side, slot] if slot else meta_out[side, 0]
                mrows[side * SLOTS + slot:side * SLOTS + slot + 1, :] = row
        for name in NAMES:
            at, count = START[name], COUNT[name]
            n, col = iota((count * BLOCK, 4 * SLOTS), 0), iota((count * BLOCK, 4 * SLOTS), 1)
            source = (n // (count * CAP)) * SLOTS + at + (n % (count * CAP)) // CAP
            picked = jnp.dot(jnp.where(source == col, 1.0, 0.0), mrows[...], preferred_element_type=F32, precision=HIGHEST)
            mine = ((at + (n % (count * CAP)) // CAP) % 8) * 16 + (n % CAP) * 4 + mx == col
            gall[at * BLOCK:(at + count) * BLOCK, :] = jnp.broadcast_to(
                jnp.sum(jnp.where(mine, picked, 0.0), axis=1, keepdims=True), (count * BLOCK, 128))

    started = []

    def compute(name):
        at, count = START[name], COUNT[name]
        spread, gather = spreads[SIZES.index(count)], gathers[SIZES.index(count)]
        edge, run, total_rows = 2 * count * BLOCK, 2 * count * CAP, 4 * count * CAP
        if name in DIRECT:
            over_done(name, AGA)
            over_done(name, AGB)
        ag(RIGHT, AGB, name).wait_recv()
        ag(LEFT, AGA, name).wait_recv()
        fwd(RIGHT, name).wait_recv()
        fwd(LEFT, name).wait_recv()
        for pair in range(2):
            block = xbuf[2 * pair:2 * pair + 2, span(name, None)].reshape(edge, part)
            ordered = jnp.dot(spread[...], block, preferred_element_type=F32).astype(BF16)
            for q in range(QUART):
                rows[pair * run:(pair + 1) * run, q * part:(q + 1) * part] = ordered[q * run:(q + 1) * run]
        if not started:
            weights[0].wait()
            weights[1].wait()
        inputs = rows[0:total_rows, :]
        gate = jnp.dot(inputs, wg[...], preferred_element_type=F32)
        up = jnp.dot(inputs, wu[...], preferred_element_type=F32)
        hidden = (gate / (1.0 + jnp.exp(-gate)) * up).astype(BF16)
        if not started:
            weights[2].wait()
            started.append(name)
        weight = gall[at * BLOCK:(at + count) * BLOCK, 0:1]
        for q in range(QUART):
            piece_out = jnp.dot(hidden, wd[:, q * part:(q + 1) * part], preferred_element_type=F32)
            piece_out = (piece_out * weight).astype(BF16)
            for pair in range(2):
                ybuf[pair * edge + q * run:pair * edge + (q + 1) * run, :] = piece_out[pair * run:(pair + 1) * run]
        for pair in (1, 0):
            block = jnp.dot(gather[...], ybuf[pair * edge:(pair + 1) * edge, :], preferred_element_type=F32).astype(BF16)
            cbuf[2 * pair:2 * pair + 2, span(name, None)] = block.reshape(2, count, BLOCK, part)
            if pair == 1:
                rs_first(RIGHT, name).start()
                rs_first(LEFT, name).start()
        if name in DIRECT:
            to_source(name, RIGHT, AGB)
            to_source(name, LEFT, AGA)
            for slot in slots_of(name):
                if slot:
                    remote(cbuf.at[0, slot], ret.at[slot], b_send, b_recv, peer(slot, 1)).start()
                else:
                    pltpu.make_async_copy(cbuf.at[0, slot], ret.at[slot], own_sem).start()
        else:
            rs_second(RIGHT, RS2B, name).start()
            rs_second(LEFT, RS2A, name).start()

    def to_source(name, side, kind):
        half_of = span(name, kind)
        for slot in range(half_of.start, half_of.stop):
            remote(cbuf.at[1 if side else 3, slot], ret.at[SLOTS + side * NEAR + slot], x_send.at[side], p_recv,
                   peer(slot, 1, -1 if side else 1)).start()

    def reduce_first(name):
        for side, held, kind in ((RIGHT, 3, RS2A), (LEFT, 1, RS2B)):
            rs_first(side, name).wait_recv()
            mine = span(name, side)
            cbuf[held, mine] = (cbuf[held, mine].astype(F32) + rs1[mine].astype(F32)).astype(BF16)
            if name in DIRECT:
                to_source(name, side, side)
            else:
                rs_second(side, kind, name).start()

    def give_back(name):
        for side in (RIGHT, LEFT):
            rs_second(side, RS2A, name).wait_recv()
            rs_second(side, RS2B, name).wait_recv()
        all_of = span(name, None)
        total = cbuf[0, all_of].astype(F32) + rs2[RIGHT, all_of].astype(F32) + rs2[LEFT, all_of].astype(F32)
        back[all_of] = total.astype(BF16)
        for slot in slots_of(name):
            remote(back.at[slot], ret.at[slot], b_send, b_recv, peer(slot, 1)).start()

    steps = {"d": send_direct, "g": start_gather, "f": forward, "c": compute, "r": reduce_first, "b": give_back, "o": send_over}
    plain = {"m": meta_make, "k": constants, "mS": meta_send, "mU": meta_use}
    for what in ORDER:
        with jax.named_scope(what):
            plain[what]() if what in plain else steps[what[0]](what[1])

    with jax.named_scope("sent"):
        src = msgs.at[slice(1, SLOTS)]
        remote(src, src, y_send, y_recv.at[0, 0], right).wait_send()
        for side in (RIGHT, LEFT):
            src = xbuf.at[slice(0, 3)]
            remote(src, src, x_send.at[side], x_recv.at[0, 0, 0], right).wait_send()
        src = xmeta.at[:, slice(1, SLOTS)]
        remote(src, src, m_send, m_recv, right).wait_send()
        for n in range(3):
            remote(meta_out.at[0], meta_out.at[1], xm_send.at[n], xm_recv.at[n], right).wait_send()
    with jax.named_scope("back"):
        src = ret.at[slice(1, SLOTS)]
        remote(src, src, b_send, b_recv, right).wait_recv()
        src = ret.at[slice(SLOTS, SLOTS + 2 * NEAR)]
        remote(src, src, b_send, p_recv, right).wait_recv()
        pltpu.make_async_copy(cbuf.at[0, 0], ret.at[0], own_sem).wait()
        src = xbuf.at[0, slice(1, SLOTS)]
        remote(src, src, b_send, b_recv, right).wait_send()


def finish(ret_hbm, route_hbm, out_hbm, ret, route_ref, unplace, out, in_sem, out_sem):
    tokens = route_ref.shape[1]
    part = ret.shape[2]
    fetch = [pltpu.make_async_copy(route_hbm, route_ref, in_sem.at[PIECES])]
    piece = ret.shape[0] // PIECES
    for n in range(PIECES):
        some = slice(n * piece, (n + 1) * piece)
        fetch.append(pltpu.make_async_copy(ret_hbm.at[some], ret.at[some], in_sem.at[n]))
    for copy in fetch:
        copy.start()
    fetch[0].wait()
    slot_row, rank = slots_and_ranks(route_ref, tokens)
    pos_col = jnp.broadcast_to((slot_row * CAP + rank).astype(F32), (tokens, tokens)).T[:, 0:1].astype(I32)
    r = iota((tokens, SLOTS * BLOCK), 1)
    hit = (r // BLOCK) * CAP + r % CAP == pos_col
    for q in range(QUART):
        unplace[q * tokens:(q + 1) * tokens, :] = onehot(hit & ((r // CAP) % QUART == q))
    for copy in fetch[1:]:
        copy.wait()
    total = ret[0:NEAR].astype(F32) + ret[SLOTS:SLOTS + NEAR].astype(F32) + ret[SLOTS + NEAR:].astype(F32)
    ret[0:NEAR] = total.astype(BF16)
    copies = []
    for q in range(QUART):
        row = jnp.dot(unplace[q * tokens:(q + 1) * tokens, :], ret[0:SLOTS].reshape(SLOTS * BLOCK, part),
                      preferred_element_type=F32).astype(BF16)
        columns = slice(q * part, (q + 1) * part)
        out[:, columns] = row
        copies.append(pltpu.make_async_copy(out.at[:, columns], out_hbm.at[:, columns], out_sem.at[q]))
        copies[-1].start()
    for copy in copies:
        copy.wait()


def local(tokens, norm_gain, w_gate, w_up, w_down, routing, gate_weight):
    count, width = tokens.shape
    hidden = w_gate.shape[2]
    part = width // QUART
    total = SLOTS * BLOCK
    hbm = pl.BlockSpec(memory_space=pltpu.HBM)
    dma = pltpu.SemaphoreType.DMA
    returned = pl.pallas_call(
        kernel,
        out_shape=jax.ShapeDtypeStruct((SLOTS + 2 * NEAR, BLOCK, part), BF16),
        in_specs=[hbm] * 7,
        out_specs=hbm,
        scratch_shapes=[
            pltpu.VMEM((count, width), BF16),
            pltpu.VMEM((1, width), F32),
            pltpu.VMEM((2, count), I32),
            pltpu.VMEM((2, count), F32),
            pltpu.VMEM((width, hidden), BF16),
            pltpu.VMEM((width, hidden), BF16),
            pltpu.VMEM((hidden, width), BF16),
            pltpu.VMEM((QUART * count, part), BF16),
            pltpu.VMEM((total, QUART * count), BF16),
            [pltpu.VMEM((2 * size * BLOCK, 2 * size * BLOCK), BF16) for size in SIZES],
            [pltpu.VMEM((2 * size * BLOCK, 2 * size * BLOCK), BF16) for size in SIZES],
            pltpu.VMEM((SLOTS, BLOCK, part), BF16),
            pltpu.VMEM((4, SLOTS // 8, 1, 128), F32),
            pltpu.VMEM((4, SLOTS, BLOCK, part), BF16),
            pltpu.VMEM((4, SLOTS, 1, 128), F32),
            pltpu.VMEM((4 * SLOTS, 128), F32),
            pltpu.VMEM((4 * SLOTS * CAP, 128), F32),
            pltpu.VMEM((max(SIZES) * BLOCK, width), BF16),
            pltpu.VMEM((4 * max(SIZES) * BLOCK, part), BF16),
            pltpu.VMEM((4, SLOTS, BLOCK, part), BF16),
            pltpu.VMEM((SLOTS, BLOCK, part), BF16),
            pltpu.VMEM((2, SLOTS, BLOCK, part), BF16),
            pltpu.VMEM((SLOTS, BLOCK, part), BF16),
            dma((7,)), dma, dma((2, len(NAMES))), dma, dma,
            dma((2,)), dma((2, 6, len(NAMES))), dma((3,)), dma((3,)), dma, dma, dma, dma,
        ],
        compiler_params=pltpu.CompilerParams(
            collective_id=0, has_side_effects=True, vmem_limit_bytes=54 * 1024 * 1024
        ),
    )(tokens, norm_gain.reshape(1, width), w_gate, w_up, w_down, routing.T, gate_weight.T)
    return pl.pallas_call(
        finish,
        out_shape=jax.ShapeDtypeStruct((count, width), BF16),
        in_specs=[hbm] * 2,
        out_specs=hbm,
        scratch_shapes=[
            pltpu.VMEM((SLOTS + 2 * NEAR, BLOCK, part), BF16),
            pltpu.VMEM((2, count), I32),
            pltpu.VMEM((QUART * count, total), BF16),
            pltpu.VMEM((count, width), BF16),
            dma((PIECES + 1,)), dma((QUART,)),
        ],
        compiler_params=pltpu.CompilerParams(vmem_limit_bytes=54 * 1024 * 1024),
    )(returned, routing.T)


def solution(mesh):
    placed = (
        P(("ep", "tp"), None),
        P(),
        P(("ep", "tp"), None, None),
        P(("ep", "tp"), None, None),
        P(("ep", "tp"), None, None),
        P(("ep", "tp"), None),
        P(("ep", "tp"), None),
    )
    return jax.shard_map(
        local, mesh=mesh, in_specs=placed, out_specs=P(("ep", "tp"), None), check_vma=False
    )
```

```python
import functools

import jax
import jax.numpy as jnp
from jax import lax
from jax.experimental import pallas as pl
from jax.experimental.pallas import tpu as pltpu
from jax.sharding import PartitionSpec as P

MESH = pl.DeviceIdType.MESH
F32, BF16, I32 = jnp.float32, jnp.bfloat16, jnp.int32
HIGHEST = lax.Precision.HIGHEST

CHUNKS = {
    "E": ((0, 0),),
    "A": ((0, 1), (0, 3), (1, 0), (3, 0)),
    "D": ((1, 1), (3, 3), (1, 3)),
    "B": ((0, 2), (2, 0), (3, 1), (1, 2)),
    "C": ((2, 2), (2, 1), (2, 3), (3, 2)),
}
NAMES = tuple(CHUNKS)
DIRECT = "EA"
PAIRS = tuple(pair for name in NAMES for pair in CHUNKS[name])
SLOTS = 2 * len(PAIRS)
COUNT = {name: 2 * len(CHUNKS[name]) for name in NAMES}
START = {name: 2 * PAIRS.index(CHUNKS[name][0]) for name in NAMES}
CAP = 4
QUART = 4
BLOCK = CAP * QUART
AGA, AGB, FWD, RS1, RS2A, RS2B = range(6)
RIGHT, LEFT = 0, 1
PIECES = 1
NEAR = sum(COUNT[name] for name in DIRECT)
EARLY = START["B"]
SIZES = tuple(sorted(set(COUNT.values())))
ORDER = (
    "dE", "oD", "dA", "oC", "oB", "m", "k", "fE", "gD", "fA", "mS", "gC", "fD", "gB", "fC", "mU",
    "cD", "fB", "cC", "cB", "rC", "rD", "rB", "cA", "bC", "cE", "bD", "bB", "rA", "rE",
)


def iota(shape, dim):
    return lax.broadcasted_iota(I32, shape, dim)


def onehot(mask):
    return jnp.where(mask, 1.0, 0.0).astype(BF16)


def here():
    me = lax.axis_index("ep")
    return me // 8, (me // 2) % 4, me % 2


def slots_and_ranks(route_ref, tokens):
    z, y, c = here()
    group = route_ref[0:1, :] // 4
    square = jnp.broadcast_to(group.astype(F32), (tokens, tokens))
    earlier = (square.T == square) & (iota((tokens, tokens), 0) < iota((tokens, tokens), 1))
    rank = jnp.sum(jnp.where(earlier, 1, 0), axis=0, keepdims=True)
    rel = ((z + 4 - group // 8) % 4) * 4 + (y + 4 - (group // 2) % 4) % 4
    pair = jnp.zeros_like(group)
    for n, (dz, dy) in enumerate(PAIRS):
        pair = pair + jnp.where(rel == dz * 4 + dy, n, 0)
    return pair * 2 + (group + c) % 2, rank


def kernel(tok_hbm, gain_hbm, wg_hbm, wu_hbm, wd_hbm, route_hbm, gw_hbm, ret,
           tok_ref, gain_ref, route_ref, gw_ref, wg, wu, wd, stack, place, spreads, gathers, msgs, meta_out, xbuf, xmeta, mrows, gall,
           rows, ybuf, cbuf, rs1, rs2, back,
           w_sem, y_send, y_recv, m_send, m_recv, x_send, x_recv, xm_send, xm_recv, b_send, b_recv, p_recv, own_sem):
    tokens, width = tok_ref.shape
    part = width // QUART
    mx = lax.axis_index("tp")
    z, y, c = here()
    right = {"tp": (mx + 1) % 4}
    left = {"tp": (mx + 3) % 4}

    def peer(slot, sign, dx=0):
        dz, dy = PAIRS[slot // 2]
        dc = slot % 2
        group = ((z + 4 + sign * dz) % 4) * 8 + ((y + 4 + sign * dy) % 4) * 2 + (c + dc) % 2
        return {"ep": group, "tp": (mx + 4 + dx) % 4}

    def slots_of(name):
        return range(START[name], START[name] + COUNT[name])

    small = [pltpu.make_async_copy(src, dst, w_sem.at[3 + n]) for n, (src, dst) in enumerate((
        (tok_hbm, tok_ref), (gain_hbm, gain_ref), (route_hbm, route_ref), (gw_hbm, gw_ref)))]
    for copy in small:
        copy.start()
    weights = [pltpu.make_async_copy(src.at[0], dst, w_sem.at[n])
               for n, (src, dst) in enumerate(((wg_hbm, wg), (wu_hbm, wu), (wd_hbm, wd)))]

    barrier = pltpu.get_barrier_semaphore()
    for slot in range(1, SLOTS):
        pl.semaphore_signal(barrier, inc=1, device_id=peer(slot, -1), device_id_type=MESH)
    near = [slot for name in DIRECT for slot in slots_of(name) if slot]
    for slot in near:
        for dx in (1, -1):
            pl.semaphore_signal(barrier, inc=1, device_id=peer(slot, -1, dx), device_id_type=MESH)
    for side in (right, {"tp": (mx + 2) % 4}, left):
        pl.semaphore_signal(barrier, inc=1, device_id=side, device_id_type=MESH)

    small[2].wait()
    slot_row, rank = slots_and_ranks(route_ref, tokens)
    pos_row = slot_row * CAP + rank

    r = iota((SLOTS * BLOCK, tokens), 0)
    hit = (r // BLOCK) * CAP + r % CAP == pos_row
    for q in range(QUART):
        place[:, q * tokens:(q + 1) * tokens] = onehot(hit & ((r // CAP) % QUART == q))

    for copy in small[:2]:
        copy.wait()
    for copy in weights:
        copy.start()
    values = tok_ref[...].astype(F32)
    scale = lax.rsqrt(jnp.mean(values * values, axis=-1, keepdims=True) + 1e-06)
    normed = (values * scale * gain_ref[...]).astype(BF16)
    for q in range(QUART):
        stack[q * tokens:(q + 1) * tokens, :] = normed[:, q * part:(q + 1) * part]

    def put_in_order(low, high):
        block = jnp.dot(place[low * BLOCK:high * BLOCK, :], stack[...], preferred_element_type=F32)
        msgs[low:high] = block.astype(BF16).reshape(high - low, BLOCK, part)

    put_in_order(0, EARLY)
    put_in_order(EARLY, SLOTS)
    xbuf[0, 0] = msgs[0]

    with jax.named_scope("barrier"):
        pl.semaphore_wait(barrier, SLOTS + 2 + 2 * len(near))

    def remote(src, dst, send, recv, device):
        return pltpu.make_async_remote_copy(src_ref=src, dst_ref=dst, send_sem=send, recv_sem=recv,
                                            device_id=device, device_id_type=MESH)

    sides = (right, {"tp": (mx + 2) % 4}, left)
    def meta_make():
        small[3].wait()
        first, second = route_ref[0:1, :], route_ref[1:2, :]
        line = iota((128, tokens), 0)
        of_line = (jnp.where(first % 4 == line % 4, gw_ref[0:1, :], 0.0)
                   + jnp.where(second % 4 == line % 4, gw_ref[1:2, :], 0.0))
        of_line = jnp.where((slot_row % 8) * CAP + rank == line // 4, of_line, 0.0)
        chosen = jnp.where(iota((8, tokens), 0) == slot_row // 8, 1.0, 0.0)
        meta = lax.dot_general(chosen, of_line, (((1,), (1,)), ((), ())), preferred_element_type=F32, precision=HIGHEST)
        for n in range(SLOTS // 8):
            meta_out[0, n] = meta[n:n + 1, :]
        for n, side in enumerate(sides):
            remote(meta_out.at[0], meta_out.at[n + 1], xm_send.at[n], xm_recv.at[n], side).start()

    def span(name, kind):
        first_slot, count = START[name], COUNT[name]
        low, high = {None: (0, count), AGA: (0, count // 2), AGB: (count // 2, count)}[kind]
        return slice(first_slot + low, first_slot + high)

    def send_over(name):
        for slot in slots_of(name):
            if slot:
                n, upper = NAMES.index(name), int(slot >= START[name] + COUNT[name] // 2)
                remote(msgs.at[slot], xbuf.at[0, slot], y_send, y_recv.at[upper, n], peer(slot, -1)).start()

    def send_direct(name):
        n = NAMES.index(name)
        at, count = START[name], COUNT[name]
        for step in range(count):
            for side, held, slot in ((RIGHT, 1, at + step), (LEFT, 3, at + (step + count // 2) % count)):
                kind = AGA if slot < at + count // 2 else AGB
                remote(msgs.at[slot], xbuf.at[held, slot], x_send.at[side], x_recv.at[side, kind, n],
                       peer(slot, -1, -1 if side else 1)).start()
        send_over(name)

    def constants():
        for size, spread, gather in zip(SIZES, spreads, gathers):
            edge = 2 * size * BLOCK
            run = 2 * size * CAP
            a, b = iota((edge, edge), 0), iota((edge, edge), 1)
            spread[...] = onehot(((a % run) // CAP) * BLOCK + (a // run) * CAP + a % CAP == b)
            gather[...] = onehot(((b % run) // CAP) * BLOCK + (b // run) * CAP + b % CAP == a)

    def hop(side, src, dst, kind, name):
        return remote(src, dst, x_send.at[side], x_recv.at[side, kind, NAMES.index(name)], left if side else right)

    def ag(side, kind, name):
        part_of = span(name, kind)
        return hop(side, xbuf.at[0, part_of], xbuf.at[3 if side else 1, part_of], kind, name)

    def fwd(side, name):
        part_of = span(name, side)
        return hop(side, xbuf.at[3 if side else 1, part_of], xbuf.at[2, part_of], FWD, name)

    def rs_first(side, name):
        part_of = span(name, side)
        return hop(side, cbuf.at[2, part_of], rs1.at[part_of], RS1, name)

    def rs_second(side, kind, name):
        part_of = span(name, kind - RS2A)
        return hop(side, cbuf.at[1 if side else 3, part_of], rs2.at[side, part_of], kind, name)

    def over_done(name, kind):
        half_of = span(name, kind)
        if half_of.stop > 1:
            src = xbuf.at[0, slice(max(1, half_of.start), half_of.stop)]
            remote(src, src, y_send, y_recv.at[kind, NAMES.index(name)], right).wait_recv()

    def start_gather(name):
        for kind in (AGA, AGB):
            over_done(name, kind)
            ag(RIGHT, kind, name).start()
            ag(LEFT, kind, name).start()

    def forward(name):
        ag(RIGHT, AGA, name).wait_recv()
        fwd(RIGHT, name).start()
        ag(LEFT, AGB, name).wait_recv()
        fwd(LEFT, name).start()

    def meta_send():
        for n, side in enumerate(sides):
            remote(meta_out.at[0], meta_out.at[n + 1], xm_send.at[n], xm_recv.at[n], side).wait_recv()
        for slot in range(1, SLOTS):
            remote(meta_out.at[:, slot // 8], xmeta.at[:, slot], m_send, m_recv, peer(slot, -1)).start()

    def meta_use():
        src = xmeta.at[:, slice(1, SLOTS)]
        remote(src, src, m_send, m_recv, right).wait_recv()
        for side in range(4):
            for slot in range(SLOTS):
                row = xmeta[side, slot] if slot else meta_out[side, 0]
                mrows[side * SLOTS + slot:side * SLOTS + slot + 1, :] = row
        for name in NAMES:
            at, count = START[name], COUNT[name]
            n, col = iota((count * BLOCK, 4 * SLOTS), 0), iota((count * BLOCK, 4 * SLOTS), 1)
            source = (n // (count * CAP)) * SLOTS + at + (n % (count * CAP)) // CAP
            picked = jnp.dot(jnp.where(source == col, 1.0, 0.0), mrows[...], preferred_element_type=F32, precision=HIGHEST)
            mine = ((at + (n % (count * CAP)) // CAP) % 8) * 16 + (n % CAP) * 4 + mx == col
            gall[at * BLOCK:(at + count) * BLOCK, :] = jnp.broadcast_to(
                jnp.sum(jnp.where(mine, picked, 0.0), axis=1, keepdims=True), (count * BLOCK, 128))

    started = []

    def compute(name):
        at, count = START[name], COUNT[name]
        spread, gather = spreads[SIZES.index(count)], gathers[SIZES.index(count)]
        edge, run, total_rows = 2 * count * BLOCK, 2 * count * CAP, 4 * count * CAP
        if name in DIRECT:
            over_done(name, AGA)
            over_done(name, AGB)
        ag(RIGHT, AGB, name).wait_recv()
        ag(LEFT, AGA, name).wait_recv()
        fwd(RIGHT, name).wait_recv()
        fwd(LEFT, name).wait_recv()
        for pair in range(2):
            block = xbuf[2 * pair:2 * pair + 2, span(name, None)].reshape(edge, part)
            ordered = jnp.dot(spread[...], block, preferred_element_type=F32).astype(BF16)
            for q in range(QUART):
                rows[pair * run:(pair + 1) * run, q * part:(q + 1) * part] = ordered[q * run:(q + 1) * run]
        if not started:
            weights[0].wait()
            weights[1].wait()
        inputs = rows[0:total_rows, :]
        gate = jnp.dot(inputs, wg[...], preferred_element_type=F32)
        up = jnp.dot(inputs, wu[...], preferred_element_type=F32)
        hidden = (gate / (1.0 + jnp.exp(-gate)) * up).astype(BF16)
        if not started:
            weights[2].wait()
            started.append(name)
        weight = gall[at * BLOCK:(at + count) * BLOCK, 0:1]
        for q in range(QUART):
            piece_out = jnp.dot(hidden, wd[:, q * part:(q + 1) * part], preferred_element_type=F32)
            piece_out = (piece_out * weight).astype(BF16)
            for pair in range(2):
                ybuf[pair * edge + q * run:pair * edge + (q + 1) * run, :] = piece_out[pair * run:(pair + 1) * run]
        for pair in (1, 0):
            block = jnp.dot(gather[...], ybuf[pair * edge:(pair + 1) * edge, :], preferred_element_type=F32).astype(BF16)
            cbuf[2 * pair:2 * pair + 2, span(name, None)] = block.reshape(2, count, BLOCK, part)
            if pair == 1:
                rs_first(RIGHT, name).start()
                rs_first(LEFT, name).start()
        if name in DIRECT:
            to_source(name, RIGHT, AGB)
            to_source(name, LEFT, AGA)
            for slot in slots_of(name):
                if slot:
                    remote(cbuf.at[0, slot], ret.at[slot], b_send, b_recv, peer(slot, 1)).start()
                else:
                    pltpu.make_async_copy(cbuf.at[0, slot], ret.at[slot], own_sem).start()
        else:
            rs_second(RIGHT, RS2B, name).start()
            rs_second(LEFT, RS2A, name).start()

    def to_source(name, side, kind):
        half_of = span(name, kind)
        for slot in range(half_of.start, half_of.stop):
            remote(cbuf.at[1 if side else 3, slot], ret.at[SLOTS + side * NEAR + slot], x_send.at[side], p_recv,
                   peer(slot, 1, -1 if side else 1)).start()

    def reduce_first(name):
        for side, held, kind in ((RIGHT, 3, RS2A), (LEFT, 1, RS2B)):
            rs_first(side, name).wait_recv()
            mine = span(name, side)
            cbuf[held, mine] = (cbuf[held, mine].astype(F32) + rs1[mine].astype(F32)).astype(BF16)
            if name in DIRECT:
                to_source(name, side, side)
            else:
                rs_second(side, kind, name).start()

    def give_back(name):
        for side in (RIGHT, LEFT):
            rs_second(side, RS2A, name).wait_recv()
            rs_second(side, RS2B, name).wait_recv()
        all_of = span(name, None)
        total = cbuf[0, all_of].astype(F32) + rs2[RIGHT, all_of].astype(F32) + rs2[LEFT, all_of].astype(F32)
        back[all_of] = total.astype(BF16)
        for slot in slots_of(name):
            remote(back.at[slot], ret.at[slot], b_send, b_recv, peer(slot, 1)).start()

    steps = {"d": send_direct, "g": start_gather, "f": forward, "c": compute, "r": reduce_first, "b": give_back, "o": send_over}
    plain = {"m": meta_make, "k": constants, "mS": meta_send, "mU": meta_use}
    for what in ORDER:
        with jax.named_scope(what):
            plain[what]() if what in plain else steps[what[0]](what[1])

    with jax.named_scope("sent"):
        src = msgs.at[slice(1, SLOTS)]
        remote(src, src, y_send, y_recv.at[0, 0], right).wait_send()
        for side in (RIGHT, LEFT):
            src = xbuf.at[slice(0, 3)]
            remote(src, src, x_send.at[side], x_recv.at[0, 0, 0], right).wait_send()
        src = xmeta.at[:, slice(1, SLOTS)]
        remote(src, src, m_send, m_recv, right).wait_send()
        for n in range(3):
            remote(meta_out.at[0], meta_out.at[1], xm_send.at[n], xm_recv.at[n], right).wait_send()
    with jax.named_scope("back"):
        src = ret.at[slice(1, SLOTS)]
        remote(src, src, b_send, b_recv, right).wait_recv()
        src = ret.at[slice(SLOTS, SLOTS + 2 * NEAR)]
        remote(src, src, b_send, p_recv, right).wait_recv()
        pltpu.make_async_copy(cbuf.at[0, 0], ret.at[0], own_sem).wait()
        src = xbuf.at[0, slice(1, SLOTS)]
        remote(src, src, b_send, b_recv, right).wait_send()


def finish(ret_hbm, route_hbm, out_hbm, ret, route_ref, unplace, out, in_sem, out_sem):
    tokens = route_ref.shape[1]
    part = ret.shape[2]
    fetch = [pltpu.make_async_copy(route_hbm, route_ref, in_sem.at[PIECES])]
    piece = ret.shape[0] // PIECES
    for n in range(PIECES):
        some = slice(n * piece, (n + 1) * piece)
        fetch.append(pltpu.make_async_copy(ret_hbm.at[some], ret.at[some], in_sem.at[n]))
    for copy in fetch:
        copy.start()
    fetch[0].wait()
    slot_row, rank = slots_and_ranks(route_ref, tokens)
    pos_col = jnp.broadcast_to((slot_row * CAP + rank).astype(F32), (tokens, tokens)).T[:, 0:1].astype(I32)
    r = iota((tokens, SLOTS * BLOCK), 1)
    hit = (r // BLOCK) * CAP + r % CAP == pos_col
    for q in range(QUART):
        unplace[q * tokens:(q + 1) * tokens, :] = onehot(hit & ((r // CAP) % QUART == q))
    for copy in fetch[1:]:
        copy.wait()
    total = ret[0:NEAR].astype(F32) + ret[SLOTS:SLOTS + NEAR].astype(F32) + ret[SLOTS + NEAR:].astype(F32)
    ret[0:NEAR] = total.astype(BF16)
    copies = []
    for q in range(QUART):
        row = jnp.dot(unplace[q * tokens:(q + 1) * tokens, :], ret[0:SLOTS].reshape(SLOTS * BLOCK, part),
                      preferred_element_type=F32).astype(BF16)
        columns = slice(q * part, (q + 1) * part)
        out[:, columns] = row
        copies.append(pltpu.make_async_copy(out.at[:, columns], out_hbm.at[:, columns], out_sem.at[q]))
        copies[-1].start()
    for copy in copies:
        copy.wait()


def local(tokens, norm_gain, w_gate, w_up, w_down, routing, gate_weight):
    count, width = tokens.shape
    hidden = w_gate.shape[2]
    part = width // QUART
    total = SLOTS * BLOCK
    hbm = pl.BlockSpec(memory_space=pltpu.HBM)
    dma = pltpu.SemaphoreType.DMA
    returned = pl.pallas_call(
        kernel,
        out_shape=jax.ShapeDtypeStruct((SLOTS + 2 * NEAR, BLOCK, part), BF16),
        in_specs=[hbm] * 7,
        out_specs=hbm,
        scratch_shapes=[
            pltpu.VMEM((count, width), BF16),
            pltpu.VMEM((1, width), F32),
            pltpu.VMEM((2, count), I32),
            pltpu.VMEM((2, count), F32),
            pltpu.VMEM((width, hidden), BF16),
            pltpu.VMEM((width, hidden), BF16),
            pltpu.VMEM((hidden, width), BF16),
            pltpu.VMEM((QUART * count, part), BF16),
            pltpu.VMEM((total, QUART * count), BF16),
            [pltpu.VMEM((2 * size * BLOCK, 2 * size * BLOCK), BF16) for size in SIZES],
            [pltpu.VMEM((2 * size * BLOCK, 2 * size * BLOCK), BF16) for size in SIZES],
            pltpu.VMEM((SLOTS, BLOCK, part), BF16),
            pltpu.VMEM((4, SLOTS // 8, 1, 128), F32),
            pltpu.VMEM((4, SLOTS, BLOCK, part), BF16),
            pltpu.VMEM((4, SLOTS, 1, 128), F32),
            pltpu.VMEM((4 * SLOTS, 128), F32),
            pltpu.VMEM((4 * SLOTS * CAP, 128), F32),
            pltpu.VMEM((max(SIZES) * BLOCK, width), BF16),
            pltpu.VMEM((4 * max(SIZES) * BLOCK, part), BF16),
            pltpu.VMEM((4, SLOTS, BLOCK, part), BF16),
            pltpu.VMEM((SLOTS, BLOCK, part), BF16),
            pltpu.VMEM((2, SLOTS, BLOCK, part), BF16),
            pltpu.VMEM((SLOTS, BLOCK, part), BF16),
            dma((7,)), dma, dma((2, len(NAMES))), dma, dma,
            dma((2,)), dma((2, 6, len(NAMES))), dma((3,)), dma((3,)), dma, dma, dma, dma,
        ],
        compiler_params=pltpu.CompilerParams(
            collective_id=0, has_side_effects=True, vmem_limit_bytes=54 * 1024 * 1024
        ),
    )(tokens, norm_gain.reshape(1, width), w_gate, w_up, w_down, routing.T, gate_weight.T)
    return pl.pallas_call(
        finish,
        out_shape=jax.ShapeDtypeStruct((count, width), BF16),
        in_specs=[hbm] * 2,
        out_specs=hbm,
        scratch_shapes=[
            pltpu.VMEM((SLOTS + 2 * NEAR, BLOCK, part), BF16),
            pltpu.VMEM((2, count), I32),
            pltpu.VMEM((QUART * count, total), BF16),
            pltpu.VMEM((count, width), BF16),
            dma((PIECES + 1,)), dma((QUART,)),
        ],
        compiler_params=pltpu.CompilerParams(vmem_limit_bytes=54 * 1024 * 1024),
    )(returned, routing.T)


def solution(mesh):
    placed = (
        P(("ep", "tp"), None),
        P(),
        P(("ep", "tp"), None, None),
        P(("ep", "tp"), None, None),
        P(("ep", "tp"), None, None),
        P(("ep", "tp"), None),
        P(("ep", "tp"), None),
    )
    return jax.shard_map(
        local, mesh=mesh, in_specs=placed, out_specs=P(("ep", "tp"), None), check_vma=False
    )
```

```python
import functools

import jax
import jax.numpy as jnp
from jax import lax
from jax.experimental import pallas as pl
from jax.experimental.pallas import tpu as pltpu
from jax.sharding import PartitionSpec as P

MESH = pl.DeviceIdType.MESH
F32, BF16, I32 = jnp.float32, jnp.bfloat16, jnp.int32
HIGHEST = lax.Precision.HIGHEST

CHUNKS = {
    "E": ((0, 0),),
    "A": ((0, 1), (0, 3), (1, 0), (3, 0)),
    "D": ((1, 1), (3, 3), (1, 3)),
    "B": ((0, 2), (2, 0), (3, 1), (1, 2)),
    "C": ((2, 2), (2, 1), (2, 3), (3, 2)),
}
NAMES = tuple(CHUNKS)
DIRECT = "EA"
PAIRS = tuple(pair for name in NAMES for pair in CHUNKS[name])
SLOTS = 2 * len(PAIRS)
COUNT = {name: 2 * len(CHUNKS[name]) for name in NAMES}
START = {name: 2 * PAIRS.index(CHUNKS[name][0]) for name in NAMES}
CAP = 4
QUART = 4
BLOCK = CAP * QUART
AGA, AGB, FWD, RS1, RS2A, RS2B = range(6)
RIGHT, LEFT = 0, 1
PIECES = 1
NEAR = sum(COUNT[name] for name in DIRECT)
EARLY = START["B"]
SIZES = tuple(sorted(set(COUNT.values())))
ORDER = (
    "dE", "oD", "dA", "oC", "oB", "m", "k", "fE", "gD", "fA", "mS", "gC", "fD", "gB", "fC", "mU",
    "cD", "fB", "cC", "cB", "rC", "rB", "rD", "cA", "bC", "cE", "bB", "bD", "rA", "rE",
)


def iota(shape, dim):
    return lax.broadcasted_iota(I32, shape, dim)


def onehot(mask):
    return jnp.where(mask, 1.0, 0.0).astype(BF16)


def here():
    me = lax.axis_index("ep")
    return me // 8, (me // 2) % 4, me % 2


def slots_and_ranks(route_ref, tokens):
    z, y, c = here()
    group = route_ref[0:1, :] // 4
    square = jnp.broadcast_to(group.astype(F32), (tokens, tokens))
    earlier = (square.T == square) & (iota((tokens, tokens), 0) < iota((tokens, tokens), 1))
    rank = jnp.sum(jnp.where(earlier, 1, 0), axis=0, keepdims=True)
    rel = ((z + 4 - group // 8) % 4) * 4 + (y + 4 - (group // 2) % 4) % 4
    pair = jnp.zeros_like(group)
    for n, (dz, dy) in enumerate(PAIRS):
        pair = pair + jnp.where(rel == dz * 4 + dy, n, 0)
    return pair * 2 + (group + c) % 2, rank


def kernel(tok_hbm, gain_hbm, wg_hbm, wu_hbm, wd_hbm, route_hbm, gw_hbm, ret,
           tok_ref, gain_ref, route_ref, gw_ref, wg, wu, wd, stack, place, spreads, gathers, msgs, meta_out, xbuf, xmeta, mrows, gall,
           rows, ybuf, cbuf, rs1, rs2, back,
           w_sem, y_send, y_recv, m_send, m_recv, x_send, x_recv, xm_send, xm_recv, b_send, b_recv, p_recv, own_sem):
    tokens, width = tok_ref.shape
    part = width // QUART
    mx = lax.axis_index("tp")
    z, y, c = here()
    right = {"tp": (mx + 1) % 4}
    left = {"tp": (mx + 3) % 4}

    def peer(slot, sign, dx=0):
        dz, dy = PAIRS[slot // 2]
        dc = slot % 2
        group = ((z + 4 + sign * dz) % 4) * 8 + ((y + 4 + sign * dy) % 4) * 2 + (c + dc) % 2
        return {"ep": group, "tp": (mx + 4 + dx) % 4}

    def slots_of(name):
        return range(START[name], START[name] + COUNT[name])

    small = [pltpu.make_async_copy(src, dst, w_sem.at[3 + n]) for n, (src, dst) in enumerate((
        (tok_hbm, tok_ref), (gain_hbm, gain_ref), (route_hbm, route_ref), (gw_hbm, gw_ref)))]
    for copy in small:
        copy.start()
    weights = [pltpu.make_async_copy(src.at[0], dst, w_sem.at[n])
               for n, (src, dst) in enumerate(((wg_hbm, wg), (wu_hbm, wu), (wd_hbm, wd)))]

    barrier = pltpu.get_barrier_semaphore()
    for slot in range(1, SLOTS):
        pl.semaphore_signal(barrier, inc=1, device_id=peer(slot, -1), device_id_type=MESH)
    near = [slot for name in DIRECT for slot in slots_of(name) if slot]
    for slot in near:
        for dx in (1, -1):
            pl.semaphore_signal(barrier, inc=1, device_id=peer(slot, -1, dx), device_id_type=MESH)
    for side in (right, {"tp": (mx + 2) % 4}, left):
        pl.semaphore_signal(barrier, inc=1, device_id=side, device_id_type=MESH)

    small[2].wait()
    slot_row, rank = slots_and_ranks(route_ref, tokens)
    pos_row = slot_row * CAP + rank

    r = iota((SLOTS * BLOCK, tokens), 0)
    hit = (r // BLOCK) * CAP + r % CAP == pos_row
    for q in range(QUART):
        place[:, q * tokens:(q + 1) * tokens] = onehot(hit & ((r // CAP) % QUART == q))

    for copy in small[:2]:
        copy.wait()
    for copy in weights:
        copy.start()
    values = tok_ref[...].astype(F32)
    scale = lax.rsqrt(jnp.mean(values * values, axis=-1, keepdims=True) + 1e-06)
    normed = (values * scale * gain_ref[...]).astype(BF16)
    for q in range(QUART):
        stack[q * tokens:(q + 1) * tokens, :] = normed[:, q * part:(q + 1) * part]

    def put_in_order(low, high):
        block = jnp.dot(place[low * BLOCK:high * BLOCK, :], stack[...], preferred_element_type=F32)
        msgs[low:high] = block.astype(BF16).reshape(high - low, BLOCK, part)

    put_in_order(0, EARLY)
    put_in_order(EARLY, SLOTS)
    xbuf[0, 0] = msgs[0]

    with jax.named_scope("barrier"):
        pl.semaphore_wait(barrier, SLOTS + 2 + 2 * len(near))

    def remote(src, dst, send, recv, device):
        return pltpu.make_async_remote_copy(src_ref=src, dst_ref=dst, send_sem=send, recv_sem=recv,
                                            device_id=device, device_id_type=MESH)

    sides = (right, {"tp": (mx + 2) % 4}, left)
    def meta_make():
        small[3].wait()
        first, second = route_ref[0:1, :], route_ref[1:2, :]
        line = iota((128, tokens), 0)
        of_line = (jnp.where(first % 4 == line % 4, gw_ref[0:1, :], 0.0)
                   + jnp.where(second % 4 == line % 4, gw_ref[1:2, :], 0.0))
        of_line = jnp.where((slot_row % 8) * CAP + rank == line // 4, of_line, 0.0)
        chosen = jnp.where(iota((8, tokens), 0) == slot_row // 8, 1.0, 0.0)
        meta = lax.dot_general(chosen, of_line, (((1,), (1,)), ((), ())), preferred_element_type=F32, precision=HIGHEST)
        for n in range(SLOTS // 8):
            meta_out[0, n] = meta[n:n + 1, :]
        for n, side in enumerate(sides):
            remote(meta_out.at[0], meta_out.at[n + 1], xm_send.at[n], xm_recv.at[n], side).start()

    def span(name, kind):
        first_slot, count = START[name], COUNT[name]
        low, high = {None: (0, count), AGA: (0, count // 2), AGB: (count // 2, count)}[kind]
        return slice(first_slot + low, first_slot + high)

    def send_over(name):
        for slot in slots_of(name):
            if slot:
                n, upper = NAMES.index(name), int(slot >= START[name] + COUNT[name] // 2)
                remote(msgs.at[slot], xbuf.at[0, slot], y_send, y_recv.at[upper, n], peer(slot, -1)).start()

    def send_direct(name):
        n = NAMES.index(name)
        at, count = START[name], COUNT[name]
        for step in range(count):
            for side, held, slot in ((RIGHT, 1, at + step), (LEFT, 3, at + (step + count // 2) % count)):
                kind = AGA if slot < at + count // 2 else AGB
                remote(msgs.at[slot], xbuf.at[held, slot], x_send.at[side], x_recv.at[side, kind, n],
                       peer(slot, -1, -1 if side else 1)).start()
        send_over(name)

    def constants():
        for size, spread, gather in zip(SIZES, spreads, gathers):
            edge = 2 * size * BLOCK
            run = 2 * size * CAP
            a, b = iota((edge, edge), 0), iota((edge, edge), 1)
            spread[...] = onehot(((a % run) // CAP) * BLOCK + (a // run) * CAP + a % CAP == b)
            gather[...] = onehot(((b % run) // CAP) * BLOCK + (b // run) * CAP + b % CAP == a)

    def hop(side, src, dst, kind, name):
        return remote(src, dst, x_send.at[side], x_recv.at[side, kind, NAMES.index(name)], left if side else right)

    def ag(side, kind, name):
        part_of = span(name, kind)
        return hop(side, xbuf.at[0, part_of], xbuf.at[3 if side else 1, part_of], kind, name)

    def fwd(side, name):
        part_of = span(name, side)
        return hop(side, xbuf.at[3 if side else 1, part_of], xbuf.at[2, part_of], FWD, name)

    def rs_first(side, name):
        part_of = span(name, side)
        return hop(side, cbuf.at[2, part_of], rs1.at[part_of], RS1, name)

    def rs_second(side, kind, name):
        part_of = span(name, kind - RS2A)
        return hop(side, cbuf.at[1 if side else 3, part_of], rs2.at[side, part_of], kind, name)

    def over_done(name, kind):
        half_of = span(name, kind)
        if half_of.stop > 1:
            src = xbuf.at[0, slice(max(1, half_of.start), half_of.stop)]
            remote(src, src, y_send, y_recv.at[kind, NAMES.index(name)], right).wait_recv()

    def start_gather(name):
        for kind in (AGA, AGB):
            over_done(name, kind)
            ag(RIGHT, kind, name).start()
            ag(LEFT, kind, name).start()

    def forward(name):
        ag(RIGHT, AGA, name).wait_recv()
        fwd(RIGHT, name).start()
        ag(LEFT, AGB, name).wait_recv()
        fwd(LEFT, name).start()

    def meta_send():
        for n, side in enumerate(sides):
            remote(meta_out.at[0], meta_out.at[n + 1], xm_send.at[n], xm_recv.at[n], side).wait_recv()
        for slot in range(1, SLOTS):
            remote(meta_out.at[:, slot // 8], xmeta.at[:, slot], m_send, m_recv, peer(slot, -1)).start()

    def meta_use():
        src = xmeta.at[:, slice(1, SLOTS)]
        remote(src, src, m_send, m_recv, right).wait_recv()
        for side in range(4):
            for slot in range(SLOTS):
                row = xmeta[side, slot] if slot else meta_out[side, 0]
                mrows[side * SLOTS + slot:side * SLOTS + slot + 1, :] = row
        for name in NAMES:
            at, count = START[name], COUNT[name]
            n, col = iota((count * BLOCK, 4 * SLOTS), 0), iota((count * BLOCK, 4 * SLOTS), 1)
            source = (n // (count * CAP)) * SLOTS + at + (n % (count * CAP)) // CAP
            picked = jnp.dot(jnp.where(source == col, 1.0, 0.0), mrows[...], preferred_element_type=F32, precision=HIGHEST)
            mine = ((at + (n % (count * CAP)) // CAP) % 8) * 16 + (n % CAP) * 4 + mx == col
            gall[at * BLOCK:(at + count) * BLOCK, :] = jnp.broadcast_to(
                jnp.sum(jnp.where(mine, picked, 0.0), axis=1, keepdims=True), (count * BLOCK, 128))

    started = []

    def compute(name):
        at, count = START[name], COUNT[name]
        spread, gather = spreads[SIZES.index(count)], gathers[SIZES.index(count)]
        edge, run, total_rows = 2 * count * BLOCK, 2 * count * CAP, 4 * count * CAP
        if name in DIRECT:
            over_done(name, AGA)
            over_done(name, AGB)
        ag(RIGHT, AGB, name).wait_recv()
        ag(LEFT, AGA, name).wait_recv()
        fwd(RIGHT, name).wait_recv()
        fwd(LEFT, name).wait_recv()
        for pair in range(2):
            block = xbuf[2 * pair:2 * pair + 2, span(name, None)].reshape(edge, part)
            ordered = jnp.dot(spread[...], block, preferred_element_type=F32).astype(BF16)
            for q in range(QUART):
                rows[pair * run:(pair + 1) * run, q * part:(q + 1) * part] = ordered[q * run:(q + 1) * run]
        if not started:
            weights[0].wait()
            weights[1].wait()
        inputs = rows[0:total_rows, :]
        gate = jnp.dot(inputs, wg[...], preferred_element_type=F32)
        up = jnp.dot(inputs, wu[...], preferred_element_type=F32)
        hidden = (gate / (1.0 + jnp.exp(-gate)) * up).astype(BF16)
        if not started:
            weights[2].wait()
            started.append(name)
        weight = gall[at * BLOCK:(at + count) * BLOCK, 0:1]
        for q in range(QUART):
            piece_out = jnp.dot(hidden, wd[:, q * part:(q + 1) * part], preferred_element_type=F32)
            piece_out = (piece_out * weight).astype(BF16)
            for pair in range(2):
                ybuf[pair * edge + q * run:pair * edge + (q + 1) * run, :] = piece_out[pair * run:(pair + 1) * run]
        for pair in (1, 0):
            block = jnp.dot(gather[...], ybuf[pair * edge:(pair + 1) * edge, :], preferred_element_type=F32).astype(BF16)
            cbuf[2 * pair:2 * pair + 2, span(name, None)] = block.reshape(2, count, BLOCK, part)
            if pair == 1:
                rs_first(RIGHT, name).start()
                rs_first(LEFT, name).start()
        if name in DIRECT:
            to_source(name, RIGHT, AGB)
            to_source(name, LEFT, AGA)
            for slot in slots_of(name):
                if slot:
                    remote(cbuf.at[0, slot], ret.at[slot], b_send, b_recv, peer(slot, 1)).start()
                else:
                    pltpu.make_async_copy(cbuf.at[0, slot], ret.at[slot], own_sem).start()
        else:
            rs_second(RIGHT, RS2B, name).start()
            rs_second(LEFT, RS2A, name).start()

    def to_source(name, side, kind):
        half_of = span(name, kind)
        for slot in range(half_of.start, half_of.stop):
            remote(cbuf.at[1 if side else 3, slot], ret.at[SLOTS + side * NEAR + slot], x_send.at[side], p_recv,
                   peer(slot, 1, -1 if side else 1)).start()

    def reduce_first(name):
        for side, held, kind in ((RIGHT, 3, RS2A), (LEFT, 1, RS2B)):
            rs_first(side, name).wait_recv()
            mine = span(name, side)
            cbuf[held, mine] = (cbuf[held, mine].astype(F32) + rs1[mine].astype(F32)).astype(BF16)
            if name in DIRECT:
                to_source(name, side, side)
            else:
                rs_second(side, kind, name).start()

    def give_back(name):
        for side in (RIGHT, LEFT):
            rs_second(side, RS2A, name).wait_recv()
            rs_second(side, RS2B, name).wait_recv()
        all_of = span(name, None)
        total = cbuf[0, all_of].astype(F32) + rs2[RIGHT, all_of].astype(F32) + rs2[LEFT, all_of].astype(F32)
        back[all_of] = total.astype(BF16)
        for slot in slots_of(name):
            remote(back.at[slot], ret.at[slot], b_send, b_recv, peer(slot, 1)).start()

    steps = {"d": send_direct, "g": start_gather, "f": forward, "c": compute, "r": reduce_first, "b": give_back, "o": send_over}
    plain = {"m": meta_make, "k": constants, "mS": meta_send, "mU": meta_use}
    for what in ORDER:
        with jax.named_scope(what):
            plain[what]() if what in plain else steps[what[0]](what[1])

    with jax.named_scope("sent"):
        src = msgs.at[slice(1, SLOTS)]
        remote(src, src, y_send, y_recv.at[0, 0], right).wait_send()
        for side in (RIGHT, LEFT):
            src = xbuf.at[slice(0, 3)]
            remote(src, src, x_send.at[side], x_recv.at[0, 0, 0], right).wait_send()
        src = xmeta.at[:, slice(1, SLOTS)]
        remote(src, src, m_send, m_recv, right).wait_send()
        for n in range(3):
            remote(meta_out.at[0], meta_out.at[1], xm_send.at[n], xm_recv.at[n], right).wait_send()
    with jax.named_scope("back"):
        src = ret.at[slice(1, SLOTS)]
        remote(src, src, b_send, b_recv, right).wait_recv()
        src = ret.at[slice(SLOTS, SLOTS + 2 * NEAR)]
        remote(src, src, b_send, p_recv, right).wait_recv()
        pltpu.make_async_copy(cbuf.at[0, 0], ret.at[0], own_sem).wait()
        src = xbuf.at[0, slice(1, SLOTS)]
        remote(src, src, b_send, b_recv, right).wait_send()


def finish(ret_hbm, route_hbm, out_hbm, ret, route_ref, unplace, out, in_sem, out_sem):
    tokens = route_ref.shape[1]
    part = ret.shape[2]
    fetch = [pltpu.make_async_copy(route_hbm, route_ref, in_sem.at[PIECES])]
    piece = ret.shape[0] // PIECES
    for n in range(PIECES):
        some = slice(n * piece, (n + 1) * piece)
        fetch.append(pltpu.make_async_copy(ret_hbm.at[some], ret.at[some], in_sem.at[n]))
    for copy in fetch:
        copy.start()
    fetch[0].wait()
    slot_row, rank = slots_and_ranks(route_ref, tokens)
    pos_col = jnp.broadcast_to((slot_row * CAP + rank).astype(F32), (tokens, tokens)).T[:, 0:1].astype(I32)
    r = iota((tokens, SLOTS * BLOCK), 1)
    hit = (r // BLOCK) * CAP + r % CAP == pos_col
    for q in range(QUART):
        unplace[q * tokens:(q + 1) * tokens, :] = onehot(hit & ((r // CAP) % QUART == q))
    for copy in fetch[1:]:
        copy.wait()
    total = ret[0:NEAR].astype(F32) + ret[SLOTS:SLOTS + NEAR].astype(F32) + ret[SLOTS + NEAR:].astype(F32)
    ret[0:NEAR] = total.astype(BF16)
    copies = []
    for q in range(QUART):
        row = jnp.dot(unplace[q * tokens:(q + 1) * tokens, :], ret[0:SLOTS].reshape(SLOTS * BLOCK, part),
                      preferred_element_type=F32).astype(BF16)
        columns = slice(q * part, (q + 1) * part)
        out[:, columns] = row
        copies.append(pltpu.make_async_copy(out.at[:, columns], out_hbm.at[:, columns], out_sem.at[q]))
        copies[-1].start()
    for copy in copies:
        copy.wait()


def local(tokens, norm_gain, w_gate, w_up, w_down, routing, gate_weight):
    count, width = tokens.shape
    hidden = w_gate.shape[2]
    part = width // QUART
    total = SLOTS * BLOCK
    hbm = pl.BlockSpec(memory_space=pltpu.HBM)
    dma = pltpu.SemaphoreType.DMA
    returned = pl.pallas_call(
        kernel,
        out_shape=jax.ShapeDtypeStruct((SLOTS + 2 * NEAR, BLOCK, part), BF16),
        in_specs=[hbm] * 7,
        out_specs=hbm,
        scratch_shapes=[
            pltpu.VMEM((count, width), BF16),
            pltpu.VMEM((1, width), F32),
            pltpu.VMEM((2, count), I32),
            pltpu.VMEM((2, count), F32),
            pltpu.VMEM((width, hidden), BF16),
            pltpu.VMEM((width, hidden), BF16),
            pltpu.VMEM((hidden, width), BF16),
            pltpu.VMEM((QUART * count, part), BF16),
            pltpu.VMEM((total, QUART * count), BF16),
            [pltpu.VMEM((2 * size * BLOCK, 2 * size * BLOCK), BF16) for size in SIZES],
            [pltpu.VMEM((2 * size * BLOCK, 2 * size * BLOCK), BF16) for size in SIZES],
            pltpu.VMEM((SLOTS, BLOCK, part), BF16),
            pltpu.VMEM((4, SLOTS // 8, 1, 128), F32),
            pltpu.VMEM((4, SLOTS, BLOCK, part), BF16),
            pltpu.VMEM((4, SLOTS, 1, 128), F32),
            pltpu.VMEM((4 * SLOTS, 128), F32),
            pltpu.VMEM((4 * SLOTS * CAP, 128), F32),
            pltpu.VMEM((max(SIZES) * BLOCK, width), BF16),
            pltpu.VMEM((4 * max(SIZES) * BLOCK, part), BF16),
            pltpu.VMEM((4, SLOTS, BLOCK, part), BF16),
            pltpu.VMEM((SLOTS, BLOCK, part), BF16),
            pltpu.VMEM((2, SLOTS, BLOCK, part), BF16),
            pltpu.VMEM((SLOTS, BLOCK, part), BF16),
            dma((7,)), dma, dma((2, len(NAMES))), dma, dma,
            dma((2,)), dma((2, 6, len(NAMES))), dma((3,)), dma((3,)), dma, dma, dma, dma,
        ],
        compiler_params=pltpu.CompilerParams(
            collective_id=0, has_side_effects=True, vmem_limit_bytes=54 * 1024 * 1024
        ),
    )(tokens, norm_gain.reshape(1, width), w_gate, w_up, w_down, routing.T, gate_weight.T)
    return pl.pallas_call(
        finish,
        out_shape=jax.ShapeDtypeStruct((count, width), BF16),
        in_specs=[hbm] * 2,
        out_specs=hbm,
        scratch_shapes=[
            pltpu.VMEM((SLOTS + 2 * NEAR, BLOCK, part), BF16),
            pltpu.VMEM((2, count), I32),
            pltpu.VMEM((QUART * count, total), BF16),
            pltpu.VMEM((count, width), BF16),
            dma((PIECES + 1,)), dma((QUART,)),
        ],
        compiler_params=pltpu.CompilerParams(vmem_limit_bytes=54 * 1024 * 1024),
    )(returned, routing.T)


def solution(mesh):
    placed = (
        P(("ep", "tp"), None),
        P(),
        P(("ep", "tp"), None, None),
        P(("ep", "tp"), None, None),
        P(("ep", "tp"), None, None),
        P(("ep", "tp"), None),
        P(("ep", "tp"), None),
    )
    return jax.shard_map(
        local, mesh=mesh, in_specs=placed, out_specs=P(("ep", "tp"), None), check_vma=False
    )
```
